128 devices in a mesh: sp: 32 (over z, y, core), tp: 4 (over x).
Axes of the slice: x: 4, y: 4, z: 4, core: 2. Of those that a mesh axis runs over, the one named last changes fastest.
Arguments:
- tokens: bfloat16 [12288, 4096], P(('sp', 'tp')), may hold values from -10 to 10
- norm_gain: float32 [4096], replicated, may hold values from 0.1 to 1.9
- query_weight: bfloat16 [4096, 2048], P(None, 'tp'), may hold values from -0.09375 to 0.09375
- key_weight: bfloat16 [4096, 2048], P(None, 'tp'), may hold values from -0.09375 to 0.09375
- value_weight: bfloat16 [4096, 2048], P(None, 'tp'), may hold values from -0.09375 to 0.09375
- gate_weight: bfloat16 [4096, 2048], P(None, 'tp'), may hold values from -0.09375 to 0.09375
- query_gain: float32 [128], replicated, may hold values from 0.1 to 1.9
- key_gain: float32 [128], replicated, may hold values from 0.1 to 1.9
- score_offset: float32 [16], P('tp'), may hold values from -12 to -4
- out_gain: float32 [2048], P('tp'), may hold values from 0.1 to 1.9
- out_weight: bfloat16 [2048, 4096], P('tp'), may hold values from -0.125 to 0.125
Outputs:
- layer_out: bfloat16 [12288, 4096], P(('sp', 'tp'))
The draws below stay inside these ranges and needn't reach their ends.
All inputs are finite; a program needn't handle non-finite values.
Results may differ from the reference program's by a relative error of at most 0.03.
Values may be sent and summed in bfloat16 or wider, within the bound.
A program may use at most 192 MiB of HBM per device.

```python
import jax
import jax.numpy as jnp
from jax import lax

D = 4096
HEADS = 16
HEAD_DIM = 128
QBLOCK = 128
TOK_DEV = 384
SEQ = 12288
WIDTH = 2048
N_TP = 4


def draw_tokens(key, part):
    noise_key, direction_key, mean_key = jax.random.split(key, 3)
    blocks = SEQ // TOK_DEV
    noise_rows = jax.random.normal(noise_key, (SEQ, D), jnp.float32)
    block_means = jax.random.uniform(mean_key, (blocks,), jnp.float32, -1.0, 1.0)
    direction = jax.random.normal(direction_key, (D,), jnp.float32)
    row_means = jnp.repeat(block_means, TOK_DEV)
    return jnp.clip(noise_rows + row_means[:, None] * direction[None, :], -10.0, 10.0).astype(jnp.bfloat16)


def draw_score_offset(key, part):
    return jax.random.uniform(key, (HEADS,), jnp.float32, -12.0, -4.0)


def shard_levels(own_key, shape, cuts, low, largest):
    loudness = 1.0
    for dim, blocks in cuts:
        heights = jax.random.uniform(jax.random.fold_in(jax.random.fold_in(own_key, 6), dim), (blocks,), jnp.float32, low / len(cuts), largest / len(cuts))
        loudness = loudness * jnp.repeat(jnp.exp(heights), shape[dim] // blocks).reshape((-1,) + (1,) * (len(shape) - 1 - dim))
    return loudness


def normal_values(own_key, shape, deviation, reach, cuts=(), kind=jnp.bfloat16):
    values = jax.random.normal(own_key, shape, jnp.float32) * deviation
    if len(cuts) > 0:
        values = shard_levels(own_key, shape, cuts, -0.22, 0.18) * values
    return jnp.clip(values, min=-reach, max=reach).astype(kind)


def setup_inputs(seed: int = 0) -> dict:
    key_of = jax.random.split(jax.random.key(seed), 12)
    tokens = draw_tokens(jax.random.fold_in(key_of[11], 71), 0)
    norm_gain = jnp.clip(1.0 + 0.18 * jax.random.normal(key_of[1], (D,), jnp.float32), 0.1, 1.9)
    query_weight = normal_values(key_of[2], (D, WIDTH), D ** -0.5, 0.09375, ((1, 4),))
    key_weight = normal_values(key_of[3], (D, WIDTH), D ** -0.5, 0.09375, ((1, 4),))
    value_weight = normal_values(key_of[4], (D, WIDTH), D ** -0.5, 0.09375, ((1, 4),))
    gate_weight = normal_values(key_of[5], (D, WIDTH), D ** -0.5, 0.09375, ((1, 4),))
    query_gain = jnp.clip(1.0 + 0.18 * jax.random.normal(key_of[6], (HEAD_DIM,), jnp.float32), 0.1, 1.9)
    key_gain = jnp.clip(1.0 + 0.18 * jax.random.normal(key_of[7], (HEAD_DIM,), jnp.float32), 0.1, 1.9)
    score_offset = draw_score_offset(jax.random.fold_in(key_of[11], 71), 0)
    out_gain = jnp.clip(1.0 + 0.18 * jax.random.normal(key_of[9], (WIDTH,), jnp.float32), 0.1, 1.9)
    out_weight = normal_values(key_of[10], (WIDTH, D), WIDTH ** -0.5, 0.125, ((0, 4),))
    return {"tokens": tokens, "norm_gain": norm_gain, "query_weight": query_weight, "key_weight": key_weight, "value_weight": value_weight, "gate_weight": gate_weight, "query_gain": query_gain, "key_gain": key_gain, "score_offset": score_offset, "out_gain": out_gain, "out_weight": out_weight}


NORM_EPS = 1e-06

def rms_rows(inputs, gain_vec):
    inputs = inputs.astype(jnp.float32)
    scaled = inputs * lax.rsqrt(lax.optimization_barrier(jnp.mean(inputs * inputs, axis=-1, keepdims=True)) + NORM_EPS)
    return scaled * gain_vec

def reference(tokens, norm_gain, query_weight, key_weight, value_weight, gate_weight, query_gain, key_gain, score_offset, out_gain, out_weight):
    normed = rms_rows(tokens, norm_gain).astype(jnp.bfloat16)

    def project(matrix):
        return jnp.dot(normed, matrix, preferred_element_type=jnp.float32).astype(jnp.bfloat16)
    queries = rms_rows(project(query_weight).reshape(SEQ, HEADS, HEAD_DIM), query_gain).astype(jnp.bfloat16)
    key_rows = rms_rows(project(key_weight).reshape(SEQ, HEADS, HEAD_DIM), key_gain).astype(jnp.bfloat16)
    value_rows = project(value_weight).reshape(SEQ, HEADS, HEAD_DIM)
    gate_rows = project(gate_weight)
    query_heads = jnp.transpose(queries, (1, 0, 2)).astype(jnp.float32)
    key_heads = jnp.transpose(key_rows, (1, 0, 2)).astype(jnp.float32)
    value_heads = jnp.transpose(value_rows, (1, 0, 2)).astype(jnp.float32)
    positions = jnp.arange(SEQ, dtype=jnp.int32)
    score_scale = HEAD_DIM ** (-0.5)

    def one_block(block_number):
        first_row = (block_number * QBLOCK).astype(jnp.int32)
        query_block = lax.dynamic_slice_in_dim(query_heads, first_row, QBLOCK, 1)
        scores = jnp.einsum('hqd,hkd->hqk', query_block, key_heads) * score_scale + score_offset[:, None, None]
        query_pos = first_row + jnp.arange(QBLOCK, dtype=jnp.int32)
        causal = positions[None, None, :] < query_pos[None, :, None]
        fail_log = jnp.where(causal, jax.nn.log_sigmoid(-scores), 0.0)
        later_sum = lax.cumsum(fail_log, axis=2, reverse=True) - fail_log
        stick = jnp.where(causal, jnp.exp(jax.nn.log_sigmoid(scores) + later_sum), 0.0).astype(jnp.bfloat16)
        stick = lax.optimization_barrier(stick).astype(jnp.float32)
        return jnp.einsum('hqk,hkd->hqd', stick, value_heads)
    blocks = lax.map(one_block, jnp.arange(SEQ // QBLOCK, dtype=jnp.int32))
    attended = blocks.transpose(0, 2, 1, 3).reshape(SEQ, HEADS, HEAD_DIM).astype(jnp.bfloat16)
    normed_out = rms_rows(attended, out_gain.reshape(HEADS, HEAD_DIM)).reshape(SEQ, WIDTH)
    mixed_rows = (normed_out * jax.nn.silu(gate_rows.astype(jnp.float32))).astype(jnp.bfloat16)
    group_cols = WIDTH // N_TP
    summed = jnp.zeros((SEQ, D), jnp.float32)
    for group in range(N_TP):
        partial_value = jnp.dot(mixed_rows[:, group * group_cols:(group + 1) * group_cols], out_weight[group * group_cols:(group + 1) * group_cols], preferred_element_type=jnp.float32).astype(jnp.bfloat16)
        summed = summed + lax.optimization_barrier(partial_value).astype(jnp.float32)
    return summed.astype(jnp.bfloat16)
```

```python
import functools

import jax
import jax.numpy as jnp
from jax import lax
from jax.experimental import pallas as pl
from jax.experimental.pallas import tpu as pltpu
from jax.sharding import Mesh
from jax.sharding import PartitionSpec as P

SP = ("sp_0", "sp_1", "sp_2")
SP_TP = ("sp_0", "sp_1", "sp_2", "tp")
NORM_EPS = 1e-06

NQ = 384
KS = 512
KP = 256
LOG2E = 1.4426950408889634

def attention_kernel(blocks_of, q_ref, off_ref, ka_ref, kb_ref, va_ref, vb_ref, tri_ref, o_ref, acc_ref, carry_ref):
    off = off_ref[0]
    blks = blocks_of()
    for i in range(4):
        b = blks[i]
        acc_ref[...] = jnp.zeros_like(acc_ref)
        carry_ref[...] = jnp.zeros_like(carry_ref)
        n_hi = (b * NQ + NQ + KS - 1) // KS
        n_lo = (b * NQ) // KS
        def step(k, masked, i=i, b=b):
            start = pl.multiple_of(k * KP, KP)
            q = q_ref[i]
            ka = ka_ref[pl.ds(start, KP), :]
            kb = kb_ref[pl.ds(start, KP), :]
            dn = (((1,), (1,)), ((), ()))
            ea = jnp.exp2(lax.dot_general(q, ka, dn, preferred_element_type=jnp.float32) + off)
            eb = jnp.exp2(lax.dot_general(q, kb, dn, preferred_element_type=jnp.float32) + off)
            if masked:
                row = lax.broadcasted_iota(jnp.int32, (NQ, KP), 0) + b * NQ
                col = lax.broadcasted_iota(jnp.int32, (NQ, KP), 1) * 2 + k * KS
                ea = jnp.where(col < row, ea, 0.0)
                eb = jnp.where(col + 1 < row, eb, 0.0)
            ta = 1.0 + ea
            l = jnp.log2(ta * (1.0 + eb)).astype(jnp.bfloat16)
            eb = eb * ta
            s = jnp.dot(l, tri_ref[...], preferred_element_type=jnp.float32)
            g = jnp.exp2(s)
            wa = (ea * g).astype(jnp.bfloat16)
            wb = (eb * g).astype(jnp.bfloat16)
            part = jnp.dot(wa, va_ref[pl.ds(start, KP), :], preferred_element_type=jnp.float32)
            part += jnp.dot(wb, vb_ref[pl.ds(start, KP), :], preferred_element_type=jnp.float32)
            carry = carry_ref[...]
            acc_ref[...] += part * jnp.exp2(carry)
            carry_ref[...] = carry + jnp.broadcast_to(s[:, 0:1], (NQ, 128))
        lax.fori_loop(0, n_hi - n_lo, lambda t, c: (step(n_hi - 1 - t, True), c)[1], 0)
        lax.fori_loop(0, n_lo, lambda t, c: (step(n_lo - 1 - t, False), c)[1], 0)
        o_ref[i] = acc_ref[...].astype(o_ref.dtype)

def attention(q, off, ka, kb, va, vb, blocks_of):
    tri = -jnp.tril(jnp.ones((KP, KP), jnp.bfloat16))
    vm = pl.BlockSpec(memory_space=pltpu.VMEM)
    return pl.pallas_call(
        functools.partial(attention_kernel, blocks_of),
        out_shape=jax.ShapeDtypeStruct(q.shape, jnp.bfloat16),
        in_specs=[vm, pl.BlockSpec(memory_space=pltpu.SMEM)] + [vm] * 5,
        out_specs=vm,
        scratch_shapes=[pltpu.VMEM((NQ, 128), jnp.float32), pltpu.VMEM((NQ, 128), jnp.float32)],
        compiler_params=pltpu.CompilerParams(vmem_limit_bytes=50 * 2**20),
    )(q, off, ka, kb, va, vb, tri)


def rms_rows(inputs, gain_vec):
    inputs = inputs.astype(jnp.float32)
    scaled = inputs * lax.rsqrt(jnp.mean(inputs * inputs, axis=-1, keepdims=True) + NORM_EPS)
    return scaled * gain_vec


def own_blocks():
    group = lax.axis_index("sp_1") * 2 + lax.axis_index("sp_2")
    return [group + 8 * k for k in range(4)]


def on_device(tokens, norm_gain, query_weight, key_weight, value_weight, gate_weight, query_gain, key_gain, score_offset, out_gain, out_weight):
    normed = rms_rows(tokens, norm_gain).astype(jnp.bfloat16)
    rows = lax.all_gather(normed, "tp", axis=0, tiled=True)

    def project(matrix):
        return jnp.dot(rows, matrix, preferred_element_type=jnp.float32).astype(jnp.bfloat16)

    def heads(x):
        return x.reshape(NQ, 4, 128)

    queries = rms_rows(heads(project(query_weight)), query_gain * (LOG2E * 128**-0.5)).astype(jnp.bfloat16)
    keys = rms_rows(heads(project(key_weight)), key_gain).astype(jnp.bfloat16)
    values = heads(project(value_weight))
    gates = project(gate_weight)
    keys, values = (x.reshape(NQ // 2, 2, 4, 128).transpose(2, 1, 0, 3).reshape(4, NQ, 128) for x in (keys, values))
    packed = jnp.stack([queries.transpose(1, 0, 2), keys, values], axis=1)
    packed = lax.all_to_all(packed, "sp_0", split_axis=0, concat_axis=0, tiled=True)
    queries = packed[:, 0]
    both = lax.all_gather(packed[:, 1:], ("sp_1", "sp_2"))
    both = both.reshape(8, 4, 2, 2, NQ // 2, 128).transpose(2, 3, 1, 0, 4, 5).reshape(2, 2, 6144, 128)
    offset = (lax.dynamic_slice_in_dim(score_offset, lax.axis_index("sp_0"), 1) * LOG2E).astype(jnp.float32)
    attended = attention(queries, offset, both[0, 0], both[0, 1], both[1, 0], both[1, 1], own_blocks)
    attended = lax.all_to_all(attended, "sp_0", split_axis=0, concat_axis=0, tiled=True)
    attended = attended.transpose(1, 0, 2)
    normed_out = rms_rows(attended, out_gain.reshape(4, 128)).reshape(NQ, 512)
    mixed = (normed_out * jax.nn.silu(gates.astype(jnp.float32))).astype(jnp.bfloat16)
    partial = jnp.dot(mixed, out_weight, preferred_element_type=jnp.float32).astype(jnp.bfloat16)
    arrived = lax.all_to_all(partial.reshape(4, 96, 4096), "tp", split_axis=0, concat_axis=0, tiled=True)
    return arrived.astype(jnp.float32).sum(axis=0).astype(jnp.bfloat16)


def solution(mesh):
    finer = Mesh(mesh.devices.reshape(4, 4, 2, mesh.shape["tp"]), ("sp_0", "sp_1", "sp_2", "tp"))
    in_specs = (P(SP_TP, None), P(), P(None, "tp"), P(None, "tp"), P(None, "tp"), P(None, "tp"), P(), P(), P("tp"), P("tp"), P("tp", None))
    return jax.shard_map(on_device, mesh=finer, in_specs=in_specs, out_specs=P(SP_TP, None), check_vma=False)
```

```python
import functools

import jax
import jax.numpy as jnp
from jax import lax
from jax.experimental import pallas as pl
from jax.experimental.pallas import tpu as pltpu
from jax.sharding import Mesh
from jax.sharding import PartitionSpec as P

SP = ("sp_0", "sp_1", "sp_2")
SP_TP = ("sp_0", "sp_1", "sp_2", "tp")
NORM_EPS = 1e-06

NQ = 384
KS = 512
KP = 256
LOG2E = 1.4426950408889634

def attention_kernel(blocks_of, q_ref, off_ref, kv_ref, tri_ref, o_ref, acc_ref, carry_ref):
    off = off_ref[0]
    blks = blocks_of()
    for i in range(4):
        b = blks[i]
        acc_ref[...] = jnp.zeros_like(acc_ref)
        carry_ref[...] = jnp.zeros_like(carry_ref)
        n_hi = (b * NQ + NQ + KS - 1) // KS
        n_lo = (b * NQ) // KS
        def step(k, masked, i=i, b=b):
            start = pl.multiple_of(k * KP, KP)
            q = q_ref[i]
            ka = kv_ref[0, pl.ds(start, KP), :]
            kb = kv_ref[1, pl.ds(start, KP), :]
            dn = (((1,), (1,)), ((), ()))
            ea = jnp.exp2(lax.dot_general(q, ka, dn, preferred_element_type=jnp.float32) + off)
            eb = jnp.exp2(lax.dot_general(q, kb, dn, preferred_element_type=jnp.float32) + off)
            if masked:
                row = lax.broadcasted_iota(jnp.int32, (NQ, KP), 0) + b * NQ
                col = lax.broadcasted_iota(jnp.int32, (NQ, KP), 1) * 2 + k * KS
                ea = jnp.where(col < row, ea, 0.0)
                eb = jnp.where(col + 1 < row, eb, 0.0)
            ta = 1.0 + ea
            l = jnp.log2(ta * (1.0 + eb)).astype(jnp.bfloat16)
            eb = eb * ta
            s = jnp.dot(l, tri_ref[...], preferred_element_type=jnp.float32)
            g = jnp.exp2(s)
            wa = (ea * g).astype(jnp.bfloat16)
            wb = (eb * g).astype(jnp.bfloat16)
            part = jnp.dot(wa, kv_ref[2, pl.ds(start, KP), :], preferred_element_type=jnp.float32)
            part += jnp.dot(wb, kv_ref[3, pl.ds(start, KP), :], preferred_element_type=jnp.float32)
            carry = carry_ref[...]
            acc_ref[...] += part * jnp.exp2(carry)
            carry_ref[...] = carry + jnp.broadcast_to(s[:, 0:1], (NQ, 128))
        lax.fori_loop(0, n_hi - n_lo, lambda t, c: (step(n_hi - 1 - t, True), c)[1], 0)
        lax.fori_loop(0, n_lo, lambda t, c: (step(n_lo - 1 - t, False), c)[1], 0)
        o_ref[i] = acc_ref[...].astype(o_ref.dtype)

def attention(q, off, kv, blocks_of):
    tri = -jnp.tril(jnp.ones((KP, KP), jnp.bfloat16))
    vm = pl.BlockSpec(memory_space=pltpu.VMEM)
    return pl.pallas_call(
        functools.partial(attention_kernel, blocks_of),
        out_shape=jax.ShapeDtypeStruct(q.shape, jnp.bfloat16),
        in_specs=[vm, pl.BlockSpec(memory_space=pltpu.SMEM)] + [vm] * 2,
        out_specs=vm,
        scratch_shapes=[pltpu.VMEM((NQ, 128), jnp.float32), pltpu.VMEM((NQ, 128), jnp.float32)],
        compiler_params=pltpu.CompilerParams(vmem_limit_bytes=50 * 2**20),
    )(q, off, kv, tri)


MESH = pl.DeviceIdType.MESH
X, Y, Z, C = "tp", "sp_1", "sp_0", "sp_2"
BATCHES = (
    ((0, 0), (0, 1), (0, 2)),
    ((1, 0), (1, 1), (2, 2)),
    ((1, 2), (2, 0), (2, 1)),
    ((3, 0), (3, 1), (3, 2)),
)


def pieces_in_runs(batch):
    runs = []
    for at, (slot, piece) in enumerate(batch):
        if runs and runs[-1][0] == slot and runs[-1][1] + runs[-1][3] == piece:
            runs[-1][3] += 1
        else:
            runs.append([slot, piece, at, 1])
    return runs


RUNS = [pieces_in_runs(batch) for batch in BATCHES]


def projection_kernel(tokens_ref, norm_gain_ref, query_gain_ref, key_gain_ref, wq_ref, wk_ref, wv_ref, wg_ref,
                      kv_ref, q_ref, gate_ref,
                      xbuf, nbuf, wbuf, skv, sq, local_sem, xs, xr, zs, zr, ys, yr, qs, qr):
    x, y, z, c = (lax.axis_index(name) for name in (X, Y, Z, C))
    weight_copies = []
    for kind, ref in enumerate((wk_ref, wv_ref, wq_ref, wg_ref)):
        for half in range(2):
            weight_copies.append(pltpu.make_async_copy(ref.at[:, pl.ds(256 * half, 256)], wbuf.at[2 * kind + half], local_sem.at[2 * kind + half]))
    token_copy = pltpu.make_async_copy(tokens_ref, xbuf.at[0], local_sem.at[8])
    token_copy.start()
    for copy in weight_copies:
        copy.start()
    right, left = {X: lax.rem(x + 1, 4)}, {X: lax.rem(x + 3, 4)}
    up, down = {Y: lax.rem(y + 1, 4)}, {Y: lax.rem(y + 3, 4)}
    sibling = {C: 1 - c}
    barrier = pltpu.get_barrier_semaphore()
    partners = [right, left, up, down, sibling]
    partners += [{Z: lax.rem(z + d, 4)} for d in range(1, 4)]
    partners += [{Z: lax.rem(z + d, 4), Y: 3 - y, C: 1 - c} for d in range(4)]
    for partner in partners:
        pl.semaphore_signal(barrier, inc=1, device_id=partner, device_id_type=MESH)
    pl.semaphore_wait(barrier, len(partners))
    token_copy.wait()

    def remote(src, dst, send, recv, target):
        return pltpu.make_async_remote_copy(src_ref=src, dst_ref=dst, send_sem=send, recv_sem=recv, device_id=target, device_id_type=MESH)

    def piece(slot, p):
        return xbuf.at[slot, pl.ds(32 * p, 32), :]

    to_right = [remote(piece(0, p), piece(1, p), xs.at[p], xr.at[p], right) for p in range(3)]
    to_left = [remote(piece(0, p), piece(2, p), xs.at[3 + p], xr.at[3 + p], left) for p in range(3)]
    for k in range(3):
        to_right[k].start()
        to_left[2 - k].start()
    far = [
        remote(piece(1, 0), piece(3, 0), xs.at[6], xr.at[6], right),
        remote(piece(1 + c, 1), piece(3, 1), xs.at[7], xr.at[7], {X: lax.rem(x + 1 + 2 * c, 4)}),
        remote(piece(2, 2), piece(3, 2), xs.at[8], xr.at[8], left),
    ]

    first = lax.broadcasted_iota(jnp.int32, (96, 96), 0)
    second = lax.broadcasted_iota(jnp.int32, (96, 96), 1)
    shuffle = jnp.where(second == jnp.where(first < 48, 2 * first, 2 * first - 95), 1.0, 0.0).astype(jnp.bfloat16)

    def place(slot):
        return lax.rem(x + (0, 3, 1, 2)[slot], 4)

    def norm_batch(batch):
        gain = norm_gain_ref[...]
        for at, (slot, p) in enumerate(batch):
            for half in range(2):
                rows = xbuf[slot, 32 * p + 16 * half : 32 * p + 16 * half + 16, :].astype(jnp.float32)
                scale = lax.rsqrt(jnp.mean(rows * rows, axis=-1, keepdims=True) + NORM_EPS)
                nbuf[32 * at + 16 * half : 32 * at + 16 * half + 16, :] = (rows * scale * gain).astype(jnp.bfloat16)

    def product(n):
        return jnp.dot(nbuf[...], wbuf[n], preferred_element_type=jnp.float32).astype(jnp.bfloat16)

    def head_norm(rows, gain_ref):
        rows = rows.astype(jnp.float32)
        return (rows * lax.rsqrt(jnp.mean(rows * rows, axis=-1, keepdims=True) + NORM_EPS) * gain_ref[...]).astype(jnp.bfloat16)

    def wait_weights(bt, n):
        if bt == 0:
            weight_copies[n].wait()

    def keys_and_values(bt):
        for half in range(2):
            for kind in range(2):
                wait_weights(bt, 2 * kind + half)
                rows = product(2 * kind + half)
                for i in range(2):
                    part = rows[:, 128 * i : 128 * i + 128]
                    if kind == 0:
                        part = head_norm(part, key_gain_ref)
                    part = jnp.dot(shuffle, part, preferred_element_type=jnp.float32).astype(jnp.bfloat16)
                    skv[bt, 2 * half + i, 2 * kind] = part[:48]
                    skv[bt, 2 * half + i, 2 * kind + 1] = part[48:]

    def queries_and_gates(bt):
        for half in range(2):
            wait_weights(bt, 4 + half)
            rows = product(4 + half)
            for i in range(2):
                sq[bt, 2 * half + i] = head_norm(rows[:, 128 * i : 128 * i + 128], query_gain_ref)
        for half in range(2):
            wait_weights(bt, 6 + half)
            rows = product(6 + half)
            for slot, p, at, count in RUNS[bt]:
                start = pl.multiple_of(96 * place(slot) + 32 * p, 32)
                gate_ref[pl.ds(start, 32 * count), 256 * half : 256 * half + 256] = rows[32 * at : 32 * (at + count)]

    mine = 2 * y + c
    group = {d: 2 * lax.rem(y + d, 4) + c for d in range(4)}
    run_of, runs = {}, []
    for bt in range(4):
        for run in RUNS[bt]:
            run_of.setdefault(bt, []).append(len(runs))
            runs.append((bt, *run))

    def window(r):
        bt, slot, p, at, count = runs[r]
        return pl.ds(pl.multiple_of(48 * place(slot) + 16 * p, 16), 16 * count)

    def query_window(r):
        bt, slot, p, at, count = runs[r]
        return pl.ds(pl.multiple_of(96 * place(slot) + 32 * p, 32), 32 * count)

    def block(r, d):
        return kv_ref.at[:, :, group[d], window(r), :]

    z_copies, up_copies, down_copies, far_copies, side_copies, q_copies = {}, {}, {}, {}, {}, {}
    zig_y = jnp.where(lax.rem(z, 2) == 1, 3 - y, y)
    zig_c = jnp.where(lax.rem(z, 2) == 1, 1 - c, c)
    for r, (bt, slot, p, at, count) in enumerate(runs):
        for d in range(1, 4):
            h = lax.rem(z + d, 4)
            z_copies[r, d] = remote(skv.at[bt, h, :, pl.ds(16 * at, 16 * count), :], kv_ref.at[:, z, mine, window(r), :], zs.at[r, d], zr.at[r, d], {Z: h})
        for d in range(4):
            h = lax.rem(z + d, 4)
            target = {Z: h, Y: zig_y, C: zig_c} if d else {Y: 3 - y, C: 1 - c}
            q_copies[r, d] = remote(sq.at[bt, h, pl.ds(32 * at, 32 * count), :], q_ref.at[z, query_window(r), :], qs.at[r, d], qr.at[r, d], target)
        up_copies[r] = remote(block(r, 0), block(r, 0), ys.at[r, 0], yr.at[r, 0], up)
        down_copies[r] = remote(block(r, 0), block(r, 0), ys.at[r, 1], yr.at[r, 1], down)
        near = kv_ref.at[:, :, 2 * lax.rem(y + 3 + 2 * c, 4) + c, window(r), :]
        far_copies[r] = remote(near, near, ys.at[r, 2], yr.at[r, 2], {Y: lax.rem(y + 1 + 2 * c, 4)})
        for d in range(4):
            side_copies[r, d] = remote(block(r, d), block(r, d), ys.at[r, 3 + d], yr.at[r, 3 + d], sibling)

    def send_z(bt):
        for r in run_of[bt]:
            for d in (2, 1, 3):
                z_copies[r, d].start()
            at, count = runs[r][3], runs[r][4]
            for kind in range(4):
                kv_ref[kind, z, mine, window(r), :] = skv[bt, z, kind, 16 * at : 16 * (at + count), :]

    def send_q(bt):
        for r in run_of[bt]:
            at, count = runs[r][3], runs[r][4]
            for d in range(1, 4):
                q_copies[r, d].start()

            @pl.when(lax.rem(z, 2) == 1)
            def _():
                q_copies[r, 0].start()

            @pl.when(lax.rem(z, 2) == 0)
            def _():
                q_ref[z, query_window(r), :] = sq[bt, z, 32 * at : 32 * (at + count), :]

    def send_y(bt):
        for r in run_of[bt]:
            for d in range(1, 4):
                z_copies[r, d].wait_recv()
            up_copies[r].start()
            down_copies[r].start()
            side_copies[r, 0].start()

    def send_far(bt):
        for r in run_of[bt]:
            up_copies[r].wait_recv()
            down_copies[r].wait_recv()
            far_copies[r].start()
            side_copies[r, 1].start()
            side_copies[r, 3].start()

    def send_last(bt):
        for r in run_of[bt]:
            far_copies[r].wait_recv()
            side_copies[r, 2].start()

    norm_batch(BATCHES[0])
    keys_and_values(0)
    send_z(0)
    queries_and_gates(0)
    send_q(0)
    to_right[0].wait_recv()
    far[0].start()
    to_left[2].wait_recv()
    far[2].start()
    to_right[1].wait_recv()
    to_left[1].wait_recv()
    far[1].start()
    norm_batch(BATCHES[1])
    send_y(0)
    keys_and_values(1)
    send_z(1)
    queries_and_gates(1)
    send_q(1)
    to_right[2].wait_recv()
    to_left[0].wait_recv()
    norm_batch(BATCHES[2])
    send_y(1)
    send_far(0)
    keys_and_values(2)
    send_z(2)
    queries_and_gates(2)
    send_q(2)
    for copy in far:
        copy.wait_recv()
    norm_batch(BATCHES[3])
    send_y(2)
    send_far(1)
    keys_and_values(3)
    send_z(3)
    send_last(0)
    queries_and_gates(3)
    send_q(3)
    send_far(2)
    send_y(3)
    send_last(1)
    send_far(3)
    send_last(2)
    send_last(3)
    for r in range(len(runs)):
        for d in range(4):
            side_copies[r, d].wait_recv()
        for d in range(1, 4):
            q_copies[r, d].wait_recv()

        @pl.when(lax.rem(z, 2) == 1)
        def _():
            q_copies[r, 0].wait_recv()
            q_copies[r, 0].wait_send()

        for d in range(1, 4):
            z_copies[r, d].wait_send()
            q_copies[r, d].wait_send()
        for d in range(4):
            side_copies[r, d].wait_send()
        up_copies[r].wait_send()
        down_copies[r].wait_send()
        far_copies[r].wait_send()
    for copy in to_right + to_left + far:
        copy.wait_send()


def projections(tokens, norm_gain, query_gain, key_gain, wq, wk, wv, wg):
    vm = pl.BlockSpec(memory_space=pltpu.VMEM)
    hbm = pl.BlockSpec(memory_space=pl.ANY)
    count = sum(len(run) for run in RUNS)
    sems = pltpu.SemaphoreType.DMA
    return pl.pallas_call(
        projection_kernel,
        out_shape=(
            jax.ShapeDtypeStruct((4, 4, 8, 192, 128), jnp.bfloat16),
            jax.ShapeDtypeStruct((4, NQ, 128), jnp.bfloat16),
            jax.ShapeDtypeStruct((NQ, 512), jnp.bfloat16),
        ),
        in_specs=[hbm, vm, vm, vm, hbm, hbm, hbm, hbm],
        out_specs=(vm, vm, vm),
        scratch_shapes=[
            pltpu.VMEM((4, 96, 4096), jnp.bfloat16),
            pltpu.VMEM((96, 4096), jnp.bfloat16),
            pltpu.VMEM((8, 4096, 256), jnp.bfloat16),
            pltpu.VMEM((4, 4, 4, 48, 128), jnp.bfloat16),
            pltpu.VMEM((4, 4, 96, 128), jnp.bfloat16),
            sems((9,)), sems((9,)), sems((9,)),
            sems((count, 4)), sems((count, 4)),
            sems((count, 7)), sems((count, 7)),
            sems((count, 4)), sems((count, 4)),
        ],
        compiler_params=pltpu.CompilerParams(collective_id=0, has_side_effects=True, vmem_limit_bytes=48 * 2**20),
    )(tokens, norm_gain.reshape(1, -1), (query_gain * (LOG2E * 128**-0.5)).reshape(1, -1), key_gain.reshape(1, -1), wq, wk, wv, wg)


def rms_rows(inputs, gain_vec):
    inputs = inputs.astype(jnp.float32)
    scaled = inputs * lax.rsqrt(jnp.mean(inputs * inputs, axis=-1, keepdims=True) + NORM_EPS)
    return scaled * gain_vec


def own_blocks():
    group = lax.axis_index("sp_1") * 2 + lax.axis_index("sp_2")
    return [group, 15 - group, 16 + group, 31 - group]


def on_device(tokens, norm_gain, query_weight, key_weight, value_weight, gate_weight, query_gain, key_gain, score_offset, out_gain, out_weight):
    kv, queries, gates = projections(tokens, norm_gain, query_gain, key_gain, query_weight, key_weight, value_weight, gate_weight)
    both = kv.reshape(4, 6144, 128)
    offset = (lax.dynamic_slice_in_dim(score_offset, lax.axis_index("sp_0"), 1) * LOG2E).astype(jnp.float32)
    attended = attention(queries, offset, both, own_blocks)
    turn = [(k, 7 - k) for k in range(8)]
    swapped = lax.ppermute(attended[1::2], ("sp_1", "sp_2"), turn)
    attended = jnp.stack([attended[0], swapped[0], attended[2], swapped[1]])
    attended = lax.all_to_all(attended, "sp_0", split_axis=0, concat_axis=0, tiled=True)
    attended = attended.transpose(1, 0, 2)
    normed_out = rms_rows(attended, out_gain.reshape(4, 128)).reshape(NQ, 512)
    mixed = (normed_out * jax.nn.silu(gates.astype(jnp.float32))).astype(jnp.bfloat16)
    partial = jnp.dot(mixed, out_weight, preferred_element_type=jnp.float32).astype(jnp.bfloat16)
    arrived = lax.all_to_all(partial.reshape(4, 96, 4096), "tp", split_axis=0, concat_axis=0, tiled=True)
    return arrived.astype(jnp.float32).sum(axis=0).astype(jnp.bfloat16)


def solution(mesh):
    finer = Mesh(mesh.devices.reshape(4, 4, 2, mesh.shape["tp"]), ("sp_0", "sp_1", "sp_2", "tp"))
    in_specs = (P(SP_TP, None), P(), P(None, "tp"), P(None, "tp"), P(None, "tp"), P(None, "tp"), P(), P(), P("tp"), P("tp"), P("tp", None))
    return jax.shard_map(on_device, mesh=finer, in_specs=in_specs, out_specs=P(SP_TP, None), check_vma=False)
```

```python
import functools

import jax
import jax.numpy as jnp
from jax import lax
from jax.experimental import pallas as pl
from jax.experimental.pallas import tpu as pltpu
from jax.sharding import Mesh
from jax.sharding import PartitionSpec as P

SP_TP = ("sp_0", "sp_1", "sp_2", "tp")
NORM_EPS = 1e-06
NQ = 384
KS = 512
KP = 256
LOG2E = 1.4426950408889634

MESH = pl.DeviceIdType.MESH
X, Y, Z, C = "tp", "sp_1", "sp_0", "sp_2"
BATCHES = (
    ((0, 0), (0, 1), (0, 2)),
    ((1, 0), (1, 1), (2, 2)),
    ((1, 2), (2, 0), (2, 1)),
    ((3, 0), (3, 1), (3, 2)),
)


def pieces_in_runs(batch):
    runs = []
    for at, (slot, piece) in enumerate(batch):
        if runs and runs[-1][0] == slot and runs[-1][1] + runs[-1][3] == piece:
            runs[-1][3] += 1
        else:
            runs.append([slot, piece, at, 1])
    return runs


RUNS = [pieces_in_runs(batch) for batch in BATCHES]


def projection_kernel(tokens_ref, norm_gain_ref, query_gain_ref, key_gain_ref, wq_ref, wk_ref, wv_ref, wg_ref, wo_ref,
                      kv_ref, q_ref, gate_ref, slice_ref,
                      xbuf, nbuf, wbuf, skv, sq, sg, local_sem, xs, xr, zs, zr, ys, yr, qs, qr, gs, gr):
    x, y, z, c = (lax.axis_index(name) for name in (X, Y, Z, C))
    weight_copies = []
    for kind, ref in enumerate((wk_ref, wv_ref, wq_ref, wg_ref)):
        for half in range(2):
            weight_copies.append(pltpu.make_async_copy(ref.at[:, pl.ds(256 * half, 256)], wbuf.at[2 * kind + half], local_sem.at[2 * kind + half]))
    token_copy = pltpu.make_async_copy(tokens_ref, xbuf.at[0], local_sem.at[8])
    token_copy.start()
    slice_copy = pltpu.make_async_copy(
        wo_ref.at[pl.ds(pl.multiple_of(128 * z + 32 * y, 32), 32), pl.ds(pl.multiple_of(2048 * c, 2048), 2048)],
        slice_ref.at[0], local_sem.at[9])
    slice_copy.start()
    for copy in weight_copies:
        copy.start()
    right, left = {X: lax.rem(x + 1, 4)}, {X: lax.rem(x + 3, 4)}
    up, down = {Y: lax.rem(y + 1, 4)}, {Y: lax.rem(y + 3, 4)}
    sibling = {C: 1 - c}
    barrier = pltpu.get_barrier_semaphore()
    partners = [right, left, up, down, sibling]
    partners += [{Z: lax.rem(z + d, 4)} for d in range(1, 4)]
    partners += [{Z: lax.rem(z + d, 4), Y: 3 - y, C: 1 - c} for d in range(4)]
    for partner in partners:
        pl.semaphore_signal(barrier, inc=1, device_id=partner, device_id_type=MESH)
    pl.semaphore_wait(barrier, len(partners))
    token_copy.wait()

    def remote(src, dst, send, recv, target):
        return pltpu.make_async_remote_copy(src_ref=src, dst_ref=dst, send_sem=send, recv_sem=recv, device_id=target, device_id_type=MESH)

    def piece(slot, p):
        return xbuf.at[slot, pl.ds(32 * p, 32), :]

    to_right = [remote(piece(0, p), piece(1, p), xs.at[p], xr.at[p], right) for p in range(3)]
    to_left = [remote(piece(0, p), piece(2, p), xs.at[3 + p], xr.at[3 + p], left) for p in range(3)]
    for k in range(3):
        to_right[k].start()
        to_left[2 - k].start()
    far = [
        remote(piece(1, 0), piece(3, 0), xs.at[6], xr.at[6], right),
        remote(piece(1 + c, 1), piece(3, 1), xs.at[7], xr.at[7], {X: lax.rem(x + 1 + 2 * c, 4)}),
        remote(piece(2, 2), piece(3, 2), xs.at[8], xr.at[8], left),
    ]

    first = lax.broadcasted_iota(jnp.int32, (96, 96), 0)
    second = lax.broadcasted_iota(jnp.int32, (96, 96), 1)
    shuffle = jnp.where(second == jnp.where(first < 48, 2 * first, 2 * first - 95), 1.0, 0.0).astype(jnp.bfloat16)

    def place(slot):
        return lax.rem(x + (0, 3, 1, 2)[slot], 4)

    def norm_batch(batch):
        gain = norm_gain_ref[...]
        for at, (slot, p) in enumerate(batch):
            for half in range(2):
                rows = xbuf[slot, 32 * p + 16 * half : 32 * p + 16 * half + 16, :].astype(jnp.float32)
                scale = lax.rsqrt(jnp.mean(rows * rows, axis=-1, keepdims=True) + NORM_EPS)
                nbuf[32 * at + 16 * half : 32 * at + 16 * half + 16, :] = (rows * scale * gain).astype(jnp.bfloat16)

    def product(n):
        return jnp.dot(nbuf[...], wbuf[n], preferred_element_type=jnp.float32).astype(jnp.bfloat16)

    def head_norm(rows, gain_ref):
        rows = rows.astype(jnp.float32)
        return (rows * lax.rsqrt(jnp.mean(rows * rows, axis=-1, keepdims=True) + NORM_EPS) * gain_ref[...]).astype(jnp.bfloat16)

    def wait_weights(bt, n):
        if bt == 0:
            weight_copies[n].wait()

    def keys_and_values(bt):
        for half in range(2):
            for kind in range(2):
                wait_weights(bt, 2 * kind + half)
                rows = product(2 * kind + half)
                for i in range(2):
                    part = rows[:, 128 * i : 128 * i + 128]
                    if kind == 0:
                        part = head_norm(part, key_gain_ref)
                    part = jnp.dot(shuffle, part, preferred_element_type=jnp.float32).astype(jnp.bfloat16)
                    skv[bt, 2 * half + i, 2 * kind] = part[:48]
                    skv[bt, 2 * half + i, 2 * kind + 1] = part[48:]

    def queries_and_gates(bt):
        for half in range(2):
            wait_weights(bt, 4 + half)
            rows = product(4 + half)
            for i in range(2):
                sq[bt, 2 * half + i] = head_norm(rows[:, 128 * i : 128 * i + 128], query_gain_ref)
        for half in range(2):
            wait_weights(bt, 6 + half)
            rows = product(6 + half)
            if bt == 0:
                gate_ref[0, :, 256 * half : 256 * half + 256] = rows
            else:
                sg[bt - 1, :, 256 * half : 256 * half + 256] = rows

    mine = 2 * y + c
    group = {d: 2 * lax.rem(y + d, 4) + c for d in range(4)}
    run_of, runs = {}, []
    for bt in range(4):
        for run in RUNS[bt]:
            run_of.setdefault(bt, []).append(len(runs))
            runs.append((bt, *run))

    def window(r):
        bt, slot, p, at, count = runs[r]
        return pl.ds(pl.multiple_of(48 * place(slot) + 16 * p, 16), 16 * count)

    def query_window(r):
        bt, slot, p, at, count = runs[r]
        return pl.ds(pl.multiple_of(96 * place(slot) + 32 * p, 32), 32 * count)

    def block(r, d):
        return kv_ref.at[:, :, group[d], window(r), :]

    z_copies, up_copies, down_copies, far_copies, side_copies, q_copies, g_copies = {}, {}, {}, {}, {}, {}, {}
    zig_y = jnp.where(lax.rem(z, 2) == 1, 3 - y, y)
    zig_c = jnp.where(lax.rem(z, 2) == 1, 1 - c, c)
    for r, (bt, slot, p, at, count) in enumerate(runs):
        for d in range(1, 4):
            h = lax.rem(z + d, 4)
            z_copies[r, d] = remote(skv.at[bt, h, :, pl.ds(16 * at, 16 * count), :], kv_ref.at[:, z, mine, window(r), :], zs.at[r, d], zr.at[r, d], {Z: h})
        for d in range(4):
            h = lax.rem(z + d, 4)
            target = {Z: h, Y: zig_y, C: zig_c} if d else {Y: 3 - y, C: 1 - c}
            q_copies[r, d] = remote(sq.at[bt, h, pl.ds(32 * at, 32 * count), :], q_ref.at[z, query_window(r), :], qs.at[r, d], qr.at[r, d], target)
        if bt:
            to_rel = (0, 1, 3, 2)[slot]
            g_copies[r] = remote(sg.at[bt - 1, pl.ds(32 * at, 32 * count), :], gate_ref.at[to_rel, pl.ds(32 * p, 32 * count), :], gs.at[r], gr.at[r], {X: place(slot)})
        up_copies[r] = remote(block(r, 0), block(r, 0), ys.at[r, 0], yr.at[r, 0], up)
        down_copies[r] = remote(block(r, 0), block(r, 0), ys.at[r, 1], yr.at[r, 1], down)
        near = kv_ref.at[:, :, 2 * lax.rem(y + 3 + 2 * c, 4) + c, window(r), :]
        far_copies[r] = remote(near, near, ys.at[r, 2], yr.at[r, 2], {Y: lax.rem(y + 1 + 2 * c, 4)})
        for d in range(4):
            side_copies[r, d] = remote(block(r, d), block(r, d), ys.at[r, 3 + d], yr.at[r, 3 + d], sibling)

    def send_z(bt):
        for r in run_of[bt]:
            for d in (2, 1, 3):
                z_copies[r, d].start()
            at, count = runs[r][3], runs[r][4]
            for kind in range(4):
                kv_ref[kind, z, mine, window(r), :] = skv[bt, z, kind, 16 * at : 16 * (at + count), :]

    def send_q(bt):
        for r in run_of[bt]:
            at, count = runs[r][3], runs[r][4]
            if bt:
                g_copies[r].start()
            for d in range(1, 4):
                q_copies[r, d].start()

            @pl.when(lax.rem(z, 2) == 1)
            def _():
                q_copies[r, 0].start()

            @pl.when(lax.rem(z, 2) == 0)
            def _():
                q_ref[z, query_window(r), :] = sq[bt, z, 32 * at : 32 * (at + count), :]

    def send_y(bt):
        for r in run_of[bt]:
            for d in range(1, 4):
                z_copies[r, d].wait_recv()
            up_copies[r].start()
            down_copies[r].start()
            side_copies[r, 0].start()

    def send_far(bt):
        for r in run_of[bt]:
            up_copies[r].wait_recv()
            down_copies[r].wait_recv()
            far_copies[r].start()
            side_copies[r, 1].start()
            side_copies[r, 3].start()

    def send_last(bt):
        for r in run_of[bt]:
            far_copies[r].wait_recv()
            side_copies[r, 2].start()

    norm_batch(BATCHES[0])
    keys_and_values(0)
    send_z(0)
    queries_and_gates(0)
    send_q(0)
    to_right[0].wait_recv()
    far[0].start()
    to_left[2].wait_recv()
    far[2].start()
    to_right[1].wait_recv()
    to_left[1].wait_recv()
    far[1].start()
    slice_copy.wait()
    slice_copies = [remote(slice_ref.at[0], slice_ref.at[(4 - d) % 4], xs.at[8 + d], xr.at[8 + d], {X: lax.rem(x + d, 4)}) for d in range(1, 4)]
    for copy in slice_copies:
        copy.start()
    norm_batch(BATCHES[1])
    send_y(0)
    keys_and_values(1)
    send_z(1)
    queries_and_gates(1)
    send_q(1)
    to_right[2].wait_recv()
    to_left[0].wait_recv()
    norm_batch(BATCHES[2])
    send_y(1)
    send_far(0)
    keys_and_values(2)
    send_z(2)
    queries_and_gates(2)
    send_q(2)
    for copy in far:
        copy.wait_recv()
    norm_batch(BATCHES[3])
    send_y(2)
    send_far(1)
    keys_and_values(3)
    send_z(3)
    send_last(0)
    queries_and_gates(3)
    send_q(3)
    send_far(2)
    send_y(3)
    send_last(1)
    send_far(3)
    send_last(2)
    send_last(3)
    for r in range(len(runs)):
        for d in range(4):
            side_copies[r, d].wait_recv()
        for d in range(1, 4):
            q_copies[r, d].wait_recv()

        @pl.when(lax.rem(z, 2) == 1)
        def _():
            q_copies[r, 0].wait_recv()
            q_copies[r, 0].wait_send()

        for d in range(1, 4):
            z_copies[r, d].wait_send()
            q_copies[r, d].wait_send()
        for d in range(4):
            side_copies[r, d].wait_send()
        up_copies[r].wait_send()
        down_copies[r].wait_send()
        far_copies[r].wait_send()
        if runs[r][0]:
            g_copies[r].wait()
    for copy in slice_copies:
        copy.wait()
    for copy in to_right + to_left + far:
        copy.wait_send()


def projections(tokens, norm_gain, query_gain, key_gain, wq, wk, wv, wg, wo):
    vm = pl.BlockSpec(memory_space=pltpu.VMEM)
    hbm = pl.BlockSpec(memory_space=pltpu.HBM)
    count = sum(len(run) for run in RUNS)
    sems = pltpu.SemaphoreType.DMA
    return pl.pallas_call(
        projection_kernel,
        out_shape=(
            jax.ShapeDtypeStruct((4, 4, 8, 192, 128), jnp.bfloat16),
            jax.ShapeDtypeStruct((4, NQ, 128), jnp.bfloat16),
            jax.ShapeDtypeStruct((4, 96, 512), jnp.bfloat16),
            jax.ShapeDtypeStruct((4, 32, 2048), jnp.bfloat16),
        ),
        in_specs=[hbm, vm, vm, vm, hbm, hbm, hbm, hbm, hbm],
        out_specs=(vm, vm, vm, vm),
        scratch_shapes=[
            pltpu.VMEM((4, 96, 4096), jnp.bfloat16),
            pltpu.VMEM((96, 4096), jnp.bfloat16),
            pltpu.VMEM((8, 4096, 256), jnp.bfloat16),
            pltpu.VMEM((4, 4, 4, 48, 128), jnp.bfloat16),
            pltpu.VMEM((4, 4, 96, 128), jnp.bfloat16),
            pltpu.VMEM((3, 96, 512), jnp.bfloat16),
            sems((10,)), sems((12,)), sems((12,)),
            sems((count, 4)), sems((count, 4)),
            sems((count, 7)), sems((count, 7)),
            sems((count, 4)), sems((count, 4)),
            sems((count,)), sems((count,)),
        ],
        compiler_params=pltpu.CompilerParams(collective_id=0, has_side_effects=True, vmem_limit_bytes=48 * 2**20),
    )(tokens, norm_gain.reshape(1, -1), (query_gain * (LOG2E * 128**-0.5)).reshape(1, -1), key_gain.reshape(1, -1), wq, wk, wv, wg, wo)


def attention_kernel(q_ref, kv_ref, gate_ref, slice_ref, gain_ref, off_ref, wo_ref, tri_ref, out_ref,
                     wbuf, att, sa, mx, so, acc_ref, carry_ref, local_sem, ws, wr, as_, ar, ms, mr):
    x, y, z, c = (lax.axis_index(name) for name in (X, Y, Z, C))
    group = 2 * y + c
    barrier = pltpu.get_barrier_semaphore()
    sibling = {C: 1 - c}
    partners = [sibling, {Y: lax.rem(y + 1, 4)}, {Y: lax.rem(y + 3, 4)}]
    for dz in range(4):
        for dx in range(4):
            there = {Z: lax.rem(z + dz, 4), X: lax.rem(x + dx, 4)}
            if dz or dx:
                partners.append(there)
            partners.append({**there, Y: 3 - y, C: 1 - c})
    for partner in partners:
        pl.semaphore_signal(barrier, inc=1, device_id=partner, device_id_type=MESH)
    half_columns = pl.ds(pl.multiple_of(2048 * c, 2048), 2048)
    own_copies = [
        pltpu.make_async_copy(wo_ref.at[pl.ds(32 * p, 32), half_columns], wbuf.at[0, p // 4, p % 4], local_sem.at[p])
        for p in range(16)
    ]
    for copy in own_copies:
        copy.start()

    def remote(src, dst, send, recv, target):
        return pltpu.make_async_remote_copy(src_ref=src, dst_ref=dst, send_sem=send, recv_sem=recv, device_id=target, device_id_type=MESH)

    others = pl.ds(1, 3)
    rows_a, rows_b = pl.ds(0, 16), pl.ds(16, 16)
    along_z = [{Z: lax.rem(z + 1, 4)}, {Z: lax.rem(z + 3, 4)}, {Z: lax.rem(z + 1 + 2 * c, 4)}]
    along_y = [{Y: lax.rem(y + 1, 4)}, {Y: lax.rem(y + 3, 4)}, {Y: lax.rem(y + 1 + 2 * c, 4)}]
    passed_z, passed_y = lax.rem(z + 3 + 2 * c, 4), lax.rem(y + 3 + 2 * c, 4)
    every = pl.ds(0, 4)

    def ring(first_src, here, passed, targets, row):
        copies = [remote(first_src, here, ws.at[row, k], wr.at[row, k], targets[k]) for k in range(2)]
        return copies + [remote(passed, passed, ws.at[row, 2], wr.at[row, 2], targets[2])]

    a1 = ring(slice_ref.at[others, rows_a], wbuf.at[others, z, y, rows_a], wbuf.at[others, passed_z, y, rows_a], along_z, 0)
    b1 = ring(slice_ref.at[others, rows_b], wbuf.at[others, z, y, rows_b], wbuf.at[others, z, passed_y, rows_b], along_y, 1)
    a2 = ring(wbuf.at[others, every, y, rows_a], wbuf.at[others, every, y, rows_a], wbuf.at[others, every, passed_y, rows_a], along_y, 2)
    b2 = ring(wbuf.at[others, z, every, rows_b], wbuf.at[others, z, every, rows_b], wbuf.at[others, passed_z, every, rows_b], along_z, 3)

    def weights_begin():
        pl.semaphore_wait(barrier, len(partners))
        for copies in (a1, b1):
            copies[0].start()
            copies[1].start()
        wbuf[1:4, z, y] = slice_ref[1:4]

    def weights_pass(first, second):
        for copies in (first, second):
            copies[0].wait_recv()
            copies[1].wait_recv()
            copies[2].start()

    def weights_turn():
        for copies in (a1, b1):
            copies[2].wait_recv()
        for copies in (a2, b2):
            copies[0].start()
            copies[1].start()

    off = off_ref[z] * LOG2E

    def steps(i, b, top, count, masked):
        def step(t, unused):
            k = top - t
            start = pl.multiple_of(k * KP, KP)
            q = q_ref[i]
            ka = kv_ref[0, pl.ds(start, KP), :]
            kb = kv_ref[1, pl.ds(start, KP), :]
            dn = (((1,), (1,)), ((), ()))
            ea = jnp.exp2(lax.dot_general(q, ka, dn, preferred_element_type=jnp.float32) + off)
            eb = jnp.exp2(lax.dot_general(q, kb, dn, preferred_element_type=jnp.float32) + off)
            if masked:
                row = lax.broadcasted_iota(jnp.int32, (NQ, KP), 0) + b * NQ
                col = lax.broadcasted_iota(jnp.int32, (NQ, KP), 1) * 2 + k * KS
                ea = jnp.where(col < row, ea, 0.0)
                eb = jnp.where(col + 1 < row, eb, 0.0)
            ta = 1.0 + ea
            l = jnp.log2(ta * (1.0 + eb)).astype(jnp.bfloat16)
            eb = eb * ta
            s = jnp.dot(l, tri_ref[...], preferred_element_type=jnp.float32)
            g = jnp.exp2(s)
            wa = (ea * g).astype(jnp.bfloat16)
            wb = (eb * g).astype(jnp.bfloat16)
            part = jnp.dot(wa, kv_ref[2, pl.ds(start, KP), :], preferred_element_type=jnp.float32)
            part += jnp.dot(wb, kv_ref[3, pl.ds(start, KP), :], preferred_element_type=jnp.float32)
            carry = carry_ref[...]
            acc_ref[...] += part * jnp.exp2(carry)
            carry_ref[...] = carry + jnp.broadcast_to(s[:, 0:1], (NQ, 128))
            return unused

        lax.fori_loop(0, count, step, 0)

    def sends(i):
        target = {Y: 3 - y, C: 1 - c} if i % 2 else {}
        out = []
        for rel in range(4):
            there = lax.rem(x + 4 - rel, 4)
            out.append(remote(sa.at[i, pl.ds(pl.multiple_of(96 * there, 32), 96), :], att.at[rel, z], as_.at[i, rel], ar.at[z, rel], {Z: i, X: there, **target}))
        return out

    def unless_own(i, rel, work):
        if rel or i % 2:
            work()
        else:
            pl.when(z != i)(work)

    for i in (3, 2, 1, 0):
        b = 8 * i + (7 - group if i % 2 else group)
        acc_ref[...] = jnp.zeros_like(acc_ref)
        carry_ref[...] = jnp.zeros_like(carry_ref)
        n_hi = (b * NQ + NQ + KS - 1) // KS
        n_lo = (b * NQ) // KS
        steps(i, b, n_hi - 1, n_hi - n_lo, True)
        if i == 3:
            weights_begin()
            steps(i, b, n_lo - 1, 7, False)
            weights_pass(a1, b1)
            steps(i, b, n_lo - 8, 4, False)
            weights_turn()
            steps(i, b, n_lo - 12, n_lo - 11, False)
        else:
            steps(i, b, n_lo - 1, n_lo, False)
        if i == 2:
            weights_pass(a2, b2)
        total = acc_ref[...]
        scale = lax.rsqrt(jnp.mean(total * total, axis=-1, keepdims=True) + NORM_EPS)
        sa[i] = (total * scale * gain_ref[z]).astype(jnp.bfloat16)
        for rel, copy in enumerate(sends(i)):
            unless_own(i, rel, copy.start)
        if i % 2 == 0:
            @pl.when(z == i)
            def _():
                att[0, z] = sa[i, pl.ds(pl.multiple_of(96 * x, 32), 96), :]

    to_sibling = [remote(mx.at[0, :, pl.ds(512 * r, 512)], mx.at[1, :, pl.ds(512 * r, 512)], ms.at[r], mr.at[r], sibling) for r in range(4)]
    for r in range(4):
        for h in range(4):
            here = att.at[r, h]
            unless_own(h, r, remote(here, here, as_.at[h, r], ar.at[h, r], sibling).wait_recv)
        for h in range(4):
            gate = gate_ref[r, :, 128 * h : 128 * h + 128].astype(jnp.float32)
            mixed = att[r, h].astype(jnp.float32) * (gate / (1.0 + jnp.exp(-gate)))
            mx[0, :, 512 * r + 128 * h : 512 * r + 128 * h + 128] = mixed.astype(jnp.bfloat16)
        to_sibling[r].start()
    for copies in (a2, b2):
        copies[2].wait_recv()
    for copy in own_copies:
        copy.wait()
    for copy in to_sibling:
        copy.wait_recv()
    backs = []
    rows = mx[...].reshape(192, 2048)
    for n in range(8):
        total = jnp.zeros((192, 256), jnp.float32)
        for r in range(4):
            weight = wbuf[r, :, :, :, 256 * n : 256 * n + 256].reshape(512, 256)
            total += jnp.dot(rows[:, 512 * r : 512 * r + 512], weight, preferred_element_type=jnp.float32)
        total = total.astype(jnp.bfloat16)
        columns = pl.ds(pl.multiple_of(2048 * c + 256 * n, 256), 256)
        so[n] = total[96:]
        back = remote(so.at[n], out_ref.at[:, columns], ms.at[4 + n], mr.at[4 + n], sibling)
        back.start()
        backs.append(back)
        out_ref[:, columns] = total[:96]
    for back in backs:
        back.wait()
    for copy in to_sibling:
        copy.wait_send()
    for i in range(4):
        for rel, copy in enumerate(sends(i)):
            unless_own(i, rel, copy.wait_send)
    for copies in (a1, b1, a2, b2):
        for copy in copies:
            copy.wait_send()


def attention(q, kv, gates, slices, offset, gain, wo):
    tri = -jnp.tril(jnp.ones((KP, KP), jnp.bfloat16))
    vm = pl.BlockSpec(memory_space=pltpu.VMEM)
    hbm = pl.BlockSpec(memory_space=pltpu.HBM)
    smem = pl.BlockSpec(memory_space=pltpu.SMEM)
    sems = pltpu.SemaphoreType.DMA
    return pl.pallas_call(
        attention_kernel,
        out_shape=jax.ShapeDtypeStruct((96, 4096), jnp.bfloat16),
        in_specs=[vm, vm, vm, vm, vm, smem, hbm, vm],
        out_specs=vm,
        scratch_shapes=[
            pltpu.VMEM((4, 4, 4, 32, 2048), jnp.bfloat16),
            pltpu.VMEM((4, 4, 96, 128), jnp.bfloat16),
            pltpu.VMEM((4, NQ, 128), jnp.bfloat16),
            pltpu.VMEM((2, 96, 2048), jnp.bfloat16),
            pltpu.VMEM((8, 96, 256), jnp.bfloat16),
            pltpu.VMEM((NQ, 128), jnp.float32),
            pltpu.VMEM((NQ, 128), jnp.float32),
            sems((16,)), sems((4, 3)), sems((4, 3)),
            sems((4, 4)), sems((4, 4)), sems((12,)), sems((12,)),
        ],
        compiler_params=pltpu.CompilerParams(collective_id=1, has_side_effects=True, vmem_limit_bytes=48 * 2**20),
    )(q, kv, gates, slices, gain.reshape(4, 1, 128), offset, wo, tri)


def on_device(tokens, norm_gain, query_weight, key_weight, value_weight, gate_weight, query_gain, key_gain, score_offset, out_gain, out_weight):
    kv, queries, gates, slices = projections(tokens, norm_gain, query_gain, key_gain, query_weight, key_weight, value_weight, gate_weight, out_weight)
    return attention(queries, kv.reshape(4, 6144, 128), gates, slices, score_offset, out_gain, out_weight)


def solution(mesh):
    finer = Mesh(mesh.devices.reshape(4, 4, 2, mesh.shape["tp"]), ("sp_0", "sp_1", "sp_2", "tp"))
    in_specs = (P(SP_TP, None), P(), P(None, "tp"), P(None, "tp"), P(None, "tp"), P(None, "tp"), P(), P(), P("tp"), P("tp"), P("tp", None))
    return jax.shard_map(on_device, mesh=finer, in_specs=in_specs, out_specs=P(SP_TP, None), check_vma=False)
```

```python
import functools

import jax
import jax.numpy as jnp
from jax import lax
from jax.experimental import pallas as pl
from jax.experimental.pallas import tpu as pltpu
from jax.sharding import Mesh
from jax.sharding import PartitionSpec as P

SP_TP = ("sp_0", "sp_1", "sp_2", "tp")
NORM_EPS = 1e-06
NQ = 384
KS = 512
KP = 256
LOG2E = 1.4426950408889634

MESH = pl.DeviceIdType.MESH
X, Y, Z, C = "tp", "sp_1", "sp_0", "sp_2"
BATCHES = (
    ((0, 0), (0, 1), (0, 2)),
    ((1, 0), (1, 1), (2, 2)),
    ((1, 2), (2, 0), (2, 1)),
    ((3, 0), (3, 1), (3, 2)),
)


def pieces_in_runs(batch):
    runs = []
    for at, (slot, piece) in enumerate(batch):
        if runs and runs[-1][0] == slot and runs[-1][1] + runs[-1][3] == piece:
            runs[-1][3] += 1
        else:
            runs.append([slot, piece, at, 1])
    return runs


RUNS = [pieces_in_runs(batch) for batch in BATCHES]


def layer_kernel(tokens_ref, norm_gain_ref, query_gain_ref, key_gain_ref, wq_ref, wk_ref, wv_ref, wg_ref, wo_ref,
                      gain_ref, off_ref, tri_ref, out_ref,
                      kv_ref, q_ref, gate_ref, slice_ref, wout, wplane, att, sa, mx, so, acc_ref, carry_ref, lbuf, abuf, bbuf,
                      xbuf, nbuf, wbuf, skv, sq, sg, local_sem, xs, xr, zs, zr, ys, yr, qs, qr, gs, gr,
                      out_sem, ws, wr, as_, ar, ms, mr):
    x, y, z, c = (lax.axis_index(name) for name in (X, Y, Z, C))
    weight_copies = []
    for kind, ref in enumerate((wk_ref, wv_ref, wq_ref, wg_ref)):
        for half in range(2):
            weight_copies.append(pltpu.make_async_copy(ref.at[:, pl.ds(256 * half, 256)], wbuf.at[2 * kind + half], local_sem.at[2 * kind + half]))
    token_copy = pltpu.make_async_copy(tokens_ref, xbuf.at[0], local_sem.at[8])
    token_copy.start()
    half_columns = pl.ds(pl.multiple_of(2048 * c, 2048), 2048)
    slice_copy = pltpu.make_async_copy(
        wo_ref.at[pl.ds(pl.multiple_of(256 + 64 * z + 16 * y, 16), 16), half_columns],
        slice_ref.at[0], local_sem.at[9])
    slice_copy.start()
    for copy in weight_copies:
        copy.start()
    own_copies = [pltpu.make_async_copy(wo_ref.at[pl.ds(0, 256), half_columns], wout.at[0, pl.ds(0, 256), :], out_sem.at[16])]
    own_copies += [
        pltpu.make_async_copy(wo_ref.at[pl.ds(256 + 16 * p, 16), half_columns], wplane.at[0, p // 4, p % 4], out_sem.at[p])
        for p in range(16)
    ]
    for copy in own_copies:
        copy.start()
    right, left = {X: lax.rem(x + 1, 4)}, {X: lax.rem(x + 3, 4)}
    up, down = {Y: lax.rem(y + 1, 4)}, {Y: lax.rem(y + 3, 4)}
    sibling = {C: 1 - c}
    barrier = pltpu.get_barrier_semaphore()
    partners = [right, left, up, down, sibling]
    for dz in range(4):
        for dx in range(4):
            there = {Z: lax.rem(z + dz, 4), X: lax.rem(x + dx, 4)}
            if dz or dx % 2 == 0:
                if dz or dx:
                    partners.append(there)
            partners.append({**there, Y: 3 - y, C: 1 - c})
    for partner in partners:
        pl.semaphore_signal(barrier, inc=1, device_id=partner, device_id_type=MESH)
    pl.semaphore_wait(barrier, len(partners))
    token_copy.wait()

    def remote(src, dst, send, recv, target):
        return pltpu.make_async_remote_copy(src_ref=src, dst_ref=dst, send_sem=send, recv_sem=recv, device_id=target, device_id_type=MESH)

    def piece(slot, p):
        return xbuf.at[slot, pl.ds(32 * p, 32), :]

    to_right = [remote(piece(0, p), piece(1, p), xs.at[p], xr.at[p], right) for p in range(3)]
    to_left = [remote(piece(0, p), piece(2, p), xs.at[3 + p], xr.at[3 + p], left) for p in range(3)]
    for k in range(3):
        to_right[k].start()
        to_left[2 - k].start()
    far = [
        remote(piece(1, 0), piece(3, 0), xs.at[6], xr.at[6], right),
        remote(piece(1 + c, 1), piece(3, 1), xs.at[7], xr.at[7], {X: lax.rem(x + 1 + 2 * c, 4)}),
        remote(piece(2, 2), piece(3, 2), xs.at[8], xr.at[8], left),
    ]

    others = pl.ds(1, 3)
    left_columns, right_columns = pl.ds(0, 1024), pl.ds(1024, 1024)
    along_z = [{Z: lax.rem(z + 1, 4)}, {Z: lax.rem(z + 3, 4)}, {Z: lax.rem(z + 1 + 2 * c, 4)}]
    along_y = [{Y: lax.rem(y + 1, 4)}, {Y: lax.rem(y + 3, 4)}, {Y: lax.rem(y + 1 + 2 * c, 4)}]
    passed_z, passed_y = lax.rem(z + 3 + 2 * c, 4), lax.rem(y + 3 + 2 * c, 4)
    every = pl.ds(0, 4)

    def ring(first_src, here, passed, targets, row):
        copies = [remote(first_src, here, ws.at[row, k], wr.at[row, k], targets[k]) for k in range(2)]
        return copies + [remote(passed, passed, ws.at[row, 2], wr.at[row, 2], targets[2])]

    a1 = ring(slice_ref.at[others, :, left_columns], wplane.at[others, z, y, :, left_columns], wplane.at[others, passed_z, y, :, left_columns], along_z, 0)
    b1 = ring(slice_ref.at[others, :, right_columns], wplane.at[others, z, y, :, right_columns], wplane.at[others, z, passed_y, :, right_columns], along_y, 1)
    a2 = ring(wplane.at[others, every, y, :, left_columns], wplane.at[others, every, y, :, left_columns], wplane.at[others, every, passed_y, :, left_columns], along_y, 2)
    b2 = ring(wplane.at[others, z, every, :, right_columns], wplane.at[others, z, every, :, right_columns], wplane.at[others, passed_z, every, :, right_columns], along_z, 3)

    x_ring = [
        remote(wout.at[0, pl.ds(0, 256), :], wout.at[3, pl.ds(0, 256), :], ws.at[4, 0], wr.at[4, 0], right),
        remote(wout.at[0, pl.ds(0, 256), :], wout.at[1, pl.ds(0, 256), :], ws.at[4, 1], wr.at[4, 1], left),
        remote(wout.at[3 - 2 * c, pl.ds(0, 256), :], wout.at[2, pl.ds(0, 256), :], ws.at[4, 2], wr.at[4, 2], {X: lax.rem(x + 1 + 2 * c, 4)}),
    ]

    first = lax.broadcasted_iota(jnp.int32, (96, 96), 0)
    second = lax.broadcasted_iota(jnp.int32, (96, 96), 1)
    shuffle = jnp.where(second == jnp.where(first < 48, 2 * first, 2 * first - 95), 1.0, 0.0).astype(jnp.bfloat16)

    def place(slot):
        return lax.rem(x + (0, 3, 1, 2)[slot], 4)

    def norm_batch(batch):
        gain = norm_gain_ref[...]
        for at, (slot, p) in enumerate(batch):
            for half in range(2):
                rows = xbuf[slot, 32 * p + 16 * half : 32 * p + 16 * half + 16, :].astype(jnp.float32)
                scale = lax.rsqrt(jnp.mean(rows * rows, axis=-1, keepdims=True) + NORM_EPS)
                nbuf[32 * at + 16 * half : 32 * at + 16 * half + 16, :] = (rows * scale * gain).astype(jnp.bfloat16)

    def product(n):
        return jnp.dot(nbuf[...], wbuf[n], preferred_element_type=jnp.float32).astype(jnp.bfloat16)

    def head_norm(rows, gain_ref, factor=1.0):
        rows = rows.astype(jnp.float32)
        return (rows * lax.rsqrt(jnp.mean(rows * rows, axis=-1, keepdims=True) + NORM_EPS) * (gain_ref[...] * factor)).astype(jnp.bfloat16)

    def wait_weights(bt, n):
        if bt == 0:
            weight_copies[n].wait()

    def keys_and_values(bt):
        for half in range(2):
            for kind in range(2):
                wait_weights(bt, 2 * kind + half)
                rows = product(2 * kind + half)
                for i in range(2):
                    part = rows[:, 128 * i : 128 * i + 128]
                    if kind == 0:
                        part = head_norm(part, key_gain_ref)
                    part = jnp.dot(shuffle, part, preferred_element_type=jnp.float32).astype(jnp.bfloat16)
                    skv[bt, 2 * half + i, 2 * kind] = part[:48]
                    skv[bt, 2 * half + i, 2 * kind + 1] = part[48:]

    def queries_and_gates(bt):
        for half in range(2):
            wait_weights(bt, 4 + half)
            rows = product(4 + half)
            for i in range(2):
                sq[bt, 2 * half + i] = head_norm(rows[:, 128 * i : 128 * i + 128], query_gain_ref, LOG2E * 128**-0.5)
        for half in range(2):
            wait_weights(bt, 6 + half)
            rows = product(6 + half)
            if bt == 0:
                gate_ref[0, :, 256 * half : 256 * half + 256] = rows
            else:
                sg[bt - 1, :, 256 * half : 256 * half + 256] = rows

    mine = 2 * y + c
    group = {d: 2 * lax.rem(y + d, 4) + c for d in range(4)}
    run_of, runs = {}, []
    for bt in range(4):
        for run in RUNS[bt]:
            run_of.setdefault(bt, []).append(len(runs))
            runs.append((bt, *run))

    def window(r):
        bt, slot, p, at, count = runs[r]
        return pl.ds(pl.multiple_of(48 * place(slot) + 16 * p, 16), 16 * count)

    def query_window(r):
        bt, slot, p, at, count = runs[r]
        return pl.ds(pl.multiple_of(96 * place(slot) + 32 * p, 32), 32 * count)

    def block(r, d):
        return kv_ref.at[:, :, group[d], window(r), :]

    z_copies, up_copies, down_copies, far_copies, side_copies, q_copies, g_copies = {}, {}, {}, {}, {}, {}, {}
    zig_y = jnp.where(lax.rem(z, 2) == 1, 3 - y, y)
    zig_c = jnp.where(lax.rem(z, 2) == 1, 1 - c, c)
    for r, (bt, slot, p, at, count) in enumerate(runs):
        for d in range(1, 4):
            h = lax.rem(z + d, 4)
            z_copies[r, d] = remote(skv.at[bt, h, :, pl.ds(16 * at, 16 * count), :], kv_ref.at[:, z, mine, window(r), :], zs.at[r, d], zr.at[r, d], {Z: h})
        for d in range(4):
            h = lax.rem(z + d, 4)
            target = {Z: h, Y: zig_y, C: zig_c} if d else {Y: 3 - y, C: 1 - c}
            q_copies[r, d] = remote(sq.at[bt, h, pl.ds(32 * at, 32 * count), :], q_ref.at[z, query_window(r), :], qs.at[r, d], qr.at[r, d], target)
        if bt:
            to_rel = (0, 1, 3, 2)[slot]
            g_copies[r] = remote(sg.at[bt - 1, pl.ds(32 * at, 32 * count), :], gate_ref.at[to_rel, pl.ds(32 * p, 32 * count), :], gs.at[r], gr.at[r], {X: place(slot)})
        up_copies[r] = remote(block(r, 0), block(r, 0), ys.at[r, 0], yr.at[r, 0], up)
        down_copies[r] = remote(block(r, 0), block(r, 0), ys.at[r, 1], yr.at[r, 1], down)
        near = kv_ref.at[:, :, 2 * lax.rem(y + 3 + 2 * c, 4) + c, window(r), :]
        far_copies[r] = remote(near, near, ys.at[r, 2], yr.at[r, 2], {Y: lax.rem(y + 1 + 2 * c, 4)})
        for d in range(4):
            side_copies[r, d] = remote(block(r, d), block(r, d), ys.at[r, 3 + d], yr.at[r, 3 + d], sibling)

    def send_z(bt):
        for r in run_of[bt]:
            for d in (2, 1, 3):
                z_copies[r, d].start()
            at, count = runs[r][3], runs[r][4]
            for kind in range(4):
                kv_ref[kind, z, mine, window(r), :] = skv[bt, z, kind, 16 * at : 16 * (at + count), :]

    def send_q(bt):
        for r in run_of[bt]:
            at, count = runs[r][3], runs[r][4]
            for d in range(1, 4):
                q_copies[r, d].start()

            @pl.when(lax.rem(z, 2) == 1)
            def _():
                q_copies[r, 0].start()

            @pl.when(lax.rem(z, 2) == 0)
            def _():
                q_ref[z, query_window(r), :] = sq[bt, z, 32 * at : 32 * (at + count), :]

    def send_y(bt):
        for r in run_of[bt]:
            for d in range(1, 4):
                z_copies[r, d].wait_recv()
            up_copies[r].start()
            down_copies[r].start()
            side_copies[r, 0].start()

    def send_far(bt):
        for r in run_of[bt]:
            up_copies[r].wait_recv()
            down_copies[r].wait_recv()
            far_copies[r].start()
            side_copies[r, 1].start()
            side_copies[r, 3].start()

    def send_last(bt):
        for r in run_of[bt]:
            far_copies[r].wait_recv()
            side_copies[r, 2].start()

    norm_batch(BATCHES[0])
    keys_and_values(0)
    send_z(0)
    queries_and_gates(0)
    send_q(0)
    to_right[0].wait_recv()
    far[0].start()
    to_left[2].wait_recv()
    far[2].start()
    send_y(0)
    to_right[1].wait_recv()
    to_left[1].wait_recv()
    far[1].start()
    norm_batch(BATCHES[1])
    keys_and_values(1)
    send_z(1)
    send_far(0)
    queries_and_gates(1)
    send_q(1)
    send_y(1)
    to_right[2].wait_recv()
    to_left[0].wait_recv()
    norm_batch(BATCHES[2])
    keys_and_values(2)
    send_z(2)
    send_far(1)
    send_last(0)
    queries_and_gates(2)
    send_q(2)
    send_y(2)
    for copy in far:
        copy.wait_recv()
    slice_copy.wait()
    slice_copies = [remote(slice_ref.at[0], slice_ref.at[(4 - d) % 4], xs.at[8 + d], xr.at[8 + d], {X: lax.rem(x + d, 4)}) for d in range(1, 4)]
    for copy in slice_copies:
        copy.start()
    norm_batch(BATCHES[3])
    keys_and_values(3)
    send_z(3)
    send_last(1)
    queries_and_gates(3)
    send_q(3)
    for copy in own_copies:
        copy.wait()
    for copy in x_ring[:2]:
        copy.start()
    for r in range(len(runs)):
        if runs[r][0]:
            g_copies[r].start()
    send_far(2)
    send_y(3)
    send_last(2)
    send_far(3)
    send_last(3)
    for r in range(len(runs)):
        for d in range(4):
            side_copies[r, d].wait_recv()
        for d in range(1, 4):
            q_copies[r, d].wait_recv()

        @pl.when(lax.rem(z, 2) == 1)
        def _():
            q_copies[r, 0].wait_recv()

    for copy in slice_copies:
        copy.wait_recv()
    def weights_begin():
        for copies in (a1, b1):
            copies[0].start()
            copies[1].start()
        wplane[1:4, z, y] = slice_ref[1:4]

    def weights_pass(first, second):
        for copies in (first, second):
            copies[0].wait_recv()
            copies[1].wait_recv()
            copies[2].start()

    def weights_turn():
        for copies in (a1, b1):
            copies[2].wait_recv()
        for copies in (a2, b2):
            copies[0].start()
            copies[1].start()
        for copy in x_ring[:2]:
            copy.wait_recv()
        x_ring[2].start()

    off = off_ref[z] * LOG2E
    kv_rows = kv_ref.reshape(4, 6144, 128)

    def keys_of(kind, start):
        return kv_rows[kind, pl.ds(start, KP), :]

    weights_begin()

    dn = (((1,), (1,)), ((), ()))

    def score(i, b, k, slot, masked):
        start = pl.multiple_of(jnp.maximum(k, 0) * KP, KP)
        q = q_ref[i]
        ea = jnp.exp2(lax.dot_general(q, keys_of(0, start), dn, preferred_element_type=jnp.float32) + off)
        eb = jnp.exp2(lax.dot_general(q, keys_of(1, start), dn, preferred_element_type=jnp.float32) + off)
        if masked:
            row = lax.broadcasted_iota(jnp.int32, (NQ, KP), 0) + b * NQ
            col = lax.broadcasted_iota(jnp.int32, (NQ, KP), 1) * 2 + k * KS
            ea = jnp.where((col < row) & (col >= 0), ea, 0.0)
            eb = jnp.where((col + 1 < row) & (col >= 0), eb, 0.0)
        ta = 1.0 + ea
        lbuf[slot] = jnp.log2(ta * (1.0 + eb)).astype(jnp.bfloat16)
        abuf[slot] = ea
        bbuf[slot] = eb * ta

    def gather(k, slot):
        start = pl.multiple_of(jnp.maximum(k, 0) * KP, KP)
        s = jnp.dot(lbuf[slot], tri_ref[...], preferred_element_type=jnp.float32)
        g = jnp.exp2(s)
        wa = (abuf[slot] * g).astype(jnp.bfloat16)
        wb = (bbuf[slot] * g).astype(jnp.bfloat16)
        part = jnp.dot(wa, keys_of(2, start), preferred_element_type=jnp.float32)
        part += jnp.dot(wb, keys_of(3, start), preferred_element_type=jnp.float32)
        carry = carry_ref[...]
        acc_ref[...] += part * jnp.exp2(carry)
        carry_ref[...] = carry + jnp.broadcast_to(s[:, 0:1], (NQ, 128))

    def two_steps(i, b, k, masked):
        score(i, b, k, 0, masked)
        score(i, b, k - 1, 1, masked)
        gather(k, 0)
        gather(k - 1, 1)

    def steps(i, b, top, count):
        def pair(t, unused):
            two_steps(i, b, top - 2 * t, False)
            return unused

        def last(t, unused):
            score(i, b, top - count + 1, 0, False)
            gather(top - count + 1, 0)
            return unused

        lax.fori_loop(0, count // 2, pair, 0)
        lax.fori_loop(0, lax.rem(count, 2), last, 0)

    def sends(i):
        target = {Y: 3 - y, C: 1 - c} if i % 2 else {}
        out = []
        for rel in range(4):
            there = lax.rem(x + 4 - rel, 4)
            out.append(remote(sa.at[i, pl.ds(pl.multiple_of(96 * there, 32), 96), :], att.at[rel, z], as_.at[i, rel], ar.at[z, rel], {Z: i, X: there, **target}))
        return out

    def unless_own(i, rel, work):
        if rel or i % 2:
            work()
        else:
            pl.when(z != i)(work)

    for i in (3, 2, 1, 0):
        b = 8 * i + (7 - mine if i % 2 else mine)
        acc_ref[...] = jnp.zeros_like(acc_ref)
        carry_ref[...] = jnp.zeros_like(carry_ref)
        n_hi = (b * NQ + NQ + KS - 1) // KS
        two_steps(i, b, n_hi - 1, True)
        if i == 3:
            steps(i, b, n_hi - 3, 8)
            weights_pass(a1, b1)
            steps(i, b, n_hi - 11, 4)
            weights_turn()
            steps(i, b, n_hi - 15, n_hi - 14)
        else:
            steps(i, b, n_hi - 3, jnp.maximum(n_hi - 2, 0))
        if i == 2:
            weights_pass(a2, b2)
        total = acc_ref[...]
        scale = lax.rsqrt(jnp.mean(total * total, axis=-1, keepdims=True) + NORM_EPS)
        sa[i] = (total * scale * gain_ref[z]).astype(jnp.bfloat16)
        for rel, copy in enumerate(sends(i)):
            unless_own(i, rel, copy.start)
        if i % 2 == 0:
            @pl.when(z == i)
            def _():
                att[0, z] = sa[i, pl.ds(pl.multiple_of(96 * x, 32), 96), :]

    for r in range(len(runs)):
        if runs[r][0]:
            g_copies[r].wait_recv()
    to_sibling = [remote(mx.at[0, :, pl.ds(512 * r, 512)], mx.at[1, :, pl.ds(512 * r, 512)], ms.at[r], mr.at[r], sibling) for r in range(4)]
    for r in range(4):
        for h in range(4):
            here = att.at[r, h]
            unless_own(h, r, remote(here, here, as_.at[h, r], ar.at[h, r], sibling).wait_recv)
        for h in range(4):
            gate = gate_ref[r, :, 128 * h : 128 * h + 128].astype(jnp.float32)
            mixed = att[r, h].astype(jnp.float32) * (gate / (1.0 + jnp.exp(-gate)))
            mx[0, :, 512 * r + 128 * h : 512 * r + 128 * h + 128] = mixed.astype(jnp.bfloat16)
        to_sibling[r].start()
    for copies in (a2, b2):
        copies[2].wait_recv()
    x_ring[2].wait_recv()
    for copy in to_sibling:
        copy.wait_recv()
    backs = []
    rows = mx[...].reshape(192, 2048)
    for n in range(8):
        total = jnp.zeros((192, 256), jnp.float32)
        for r in range(4):
            near = wout[r, :, 256 * n : 256 * n + 256]
            spread = wplane[r, :, :, :, 256 * n : 256 * n + 256].reshape(256, 256)
            total += jnp.dot(rows[:, 512 * r : 512 * r + 256], near, preferred_element_type=jnp.float32)
            total += jnp.dot(rows[:, 512 * r + 256 : 512 * r + 512], spread, preferred_element_type=jnp.float32)
        total = total.astype(jnp.bfloat16)
        columns = pl.ds(pl.multiple_of(2048 * c + 256 * n, 256), 256)
        so[n] = total[96:]
        back = remote(so.at[n], out_ref.at[:, columns], ms.at[4 + n], mr.at[4 + n], sibling)
        back.start()
        backs.append(back)
        out_ref[:, columns] = total[:96]
    for back in backs:
        back.wait()
    for copy in to_sibling:
        copy.wait_send()
    for i in range(4):
        for rel, copy in enumerate(sends(i)):
            unless_own(i, rel, copy.wait_send)
    for copies in (a1, b1, a2, b2, x_ring):
        for copy in copies:
            copy.wait_send()
    for r in range(len(runs)):
        @pl.when(lax.rem(z, 2) == 1)
        def _():
            q_copies[r, 0].wait_send()

        for d in range(1, 4):
            z_copies[r, d].wait_send()
            q_copies[r, d].wait_send()
        for d in range(4):
            side_copies[r, d].wait_send()
        up_copies[r].wait_send()
        down_copies[r].wait_send()
        far_copies[r].wait_send()
        if runs[r][0]:
            g_copies[r].wait_send()
    for copy in slice_copies + to_right + to_left + far:
        copy.wait_send()


def layer(tokens, norm_gain, query_gain, key_gain, wq, wk, wv, wg, wo, offset, gain):
    tri = -jnp.tril(jnp.ones((KP, KP), jnp.bfloat16))
    vm = pl.BlockSpec(memory_space=pltpu.VMEM)
    hbm = pl.BlockSpec(memory_space=pltpu.HBM)
    smem = pl.BlockSpec(memory_space=pltpu.SMEM)
    count = sum(len(run) for run in RUNS)
    sems = pltpu.SemaphoreType.DMA
    half, full = jnp.bfloat16, jnp.float32
    return pl.pallas_call(
        layer_kernel,
        out_shape=jax.ShapeDtypeStruct((96, 4096), jnp.bfloat16),
        in_specs=[hbm, vm, vm, vm, hbm, hbm, hbm, hbm, hbm, vm, smem, vm],
        out_specs=vm,
        scratch_shapes=[
            pltpu.VMEM((4, 4, 8, 192, 128), half),
            pltpu.VMEM((4, NQ, 128), half),
            pltpu.VMEM((4, 96, 512), half),
            pltpu.VMEM((4, 16, 2048), half),
            pltpu.VMEM((4, 256, 2048), half),
            pltpu.VMEM((4, 4, 4, 16, 2048), half),
            pltpu.VMEM((4, 4, 96, 128), half),
            pltpu.VMEM((4, NQ, 128), half),
            pltpu.VMEM((2, 96, 2048), half),
            pltpu.VMEM((8, 96, 256), half),
            pltpu.VMEM((NQ, 128), full),
            pltpu.VMEM((NQ, 128), full),
            pltpu.VMEM((2, NQ, KP), half),
            pltpu.VMEM((2, NQ, KP), full),
            pltpu.VMEM((2, NQ, KP), full),
            pltpu.VMEM((4, 96, 4096), half),
            pltpu.VMEM((96, 4096), half),
            pltpu.VMEM((8, 4096, 256), half),
            pltpu.VMEM((4, 4, 4, 48, 128), half),
            pltpu.VMEM((4, 4, 96, 128), half),
            pltpu.VMEM((3, 96, 512), half),
            sems((10,)), sems((12,)), sems((12,)),
            sems((count, 4)), sems((count, 4)),
            sems((count, 7)), sems((count, 7)),
            sems((count, 4)), sems((count, 4)),
            sems((count,)), sems((count,)),
            sems((17,)), sems((5, 3)), sems((5, 3)),
            sems((4, 4)), sems((4, 4)), sems((12,)), sems((12,)),
        ],
        compiler_params=pltpu.CompilerParams(collective_id=0, has_side_effects=True, vmem_limit_bytes=62 * 2**20),
    )(tokens, norm_gain.reshape(1, -1), query_gain.reshape(1, -1), key_gain.reshape(1, -1), wq, wk, wv, wg, wo, gain.reshape(4, 1, 128), offset, tri)


def on_device(tokens, norm_gain, query_weight, key_weight, value_weight, gate_weight, query_gain, key_gain, score_offset, out_gain, out_weight):
    return layer(tokens, norm_gain, query_gain, key_gain, query_weight, key_weight, value_weight, gate_weight, out_weight, score_offset, out_gain)


def solution(mesh):
    finer = Mesh(mesh.devices.reshape(4, 4, 2, mesh.shape["tp"]), ("sp_0", "sp_1", "sp_2", "tp"))
    in_specs = (P(SP_TP, None), P(), P(None, "tp"), P(None, "tp"), P(None, "tp"), P(None, "tp"), P(), P(), P("tp"), P("tp"), P("tp", None))
    return jax.shard_map(on_device, mesh=finer, in_specs=in_specs, out_specs=P(SP_TP, None), check_vma=False)
```

```python
import functools

import jax
import jax.numpy as jnp
from jax import lax
from jax.experimental import pallas as pl
from jax.experimental.pallas import tpu as pltpu
from jax.sharding import Mesh
from jax.sharding import PartitionSpec as P

SP_TP = ("sp_0", "sp_1", "sp_2", "tp")
NORM_EPS = 1e-06
NQ = 384
KS = 512
KP = 256
LOG2E = 1.4426950408889634

MESH = pl.DeviceIdType.MESH
X, Y, Z, C = "tp", "sp_1", "sp_0", "sp_2"
BATCHES = (
    ((0, 0), (0, 1), (0, 2)),
    ((1, 0), (1, 1), (2, 2)),
    ((1, 2), (2, 0), (2, 1)),
    ((3, 0), (3, 1), (3, 2)),
)


def pieces_in_runs(batch):
    runs = []
    for at, (slot, piece) in enumerate(batch):
        if runs and runs[-1][0] == slot and runs[-1][1] + runs[-1][3] == piece:
            runs[-1][3] += 1
        else:
            runs.append([slot, piece, at, 1])
    return runs


RUNS = [pieces_in_runs(batch) for batch in BATCHES]


def layer_kernel(tokens_ref, norm_gain_ref, query_gain_ref, key_gain_ref, wq_ref, wk_ref, wv_ref, wg_ref, wo_ref,
                      gain_ref, off_ref, out_ref,
                      kv_ref, q_ref, gate_ref, slice_ref, wout, wplane, att, sa, mx, so, acc_ref, carry_ref, lbuf, abuf, bbuf, tri_ref,
                      xbuf, nbuf, wbuf, skv, sq, sg, local_sem, xs, xr, zs, zr, ys, yr, qs, qr, gs, gr, fs, fr,
                      out_sem, ws, wr, as_, ar, ms, mr):
    x, y, z, c = (lax.axis_index(name) for name in (X, Y, Z, C))
    half_columns = pl.ds(pl.multiple_of(2048 * c, 2048), 2048)
    token_copy = pltpu.make_async_copy(tokens_ref, xbuf.at[0], local_sem.at[8])
    token_copy.start()
    right, left = {X: lax.rem(x + 1, 4)}, {X: lax.rem(x + 3, 4)}
    up, down = {Y: lax.rem(y + 1, 4)}, {Y: lax.rem(y + 3, 4)}
    sibling = {C: 1 - c}
    barrier = pltpu.get_barrier_semaphore()
    partners = [right, left, up, down, sibling]
    partners += [{Z: lax.rem(z + d, 4)} for d in range(1, 4)]
    for partner in partners:
        pl.semaphore_signal(barrier, inc=1, device_id=partner, device_id_type=MESH)
    token_copy.wait()
    weight_copies = []
    for kind, ref in enumerate((wk_ref, wv_ref, wq_ref, wg_ref)):
        for half in range(2):
            weight_copies.append(pltpu.make_async_copy(ref.at[:, pl.ds(256 * half, 256)], wbuf.at[2 * kind + half], local_sem.at[2 * kind + half]))
    for copy in weight_copies:
        copy.start()
    pl.semaphore_wait(barrier, len(partners))

    def remote(src, dst, send, recv, target):
        return pltpu.make_async_remote_copy(src_ref=src, dst_ref=dst, send_sem=send, recv_sem=recv, device_id=target, device_id_type=MESH)

    def piece(slot, p):
        return xbuf.at[slot, pl.ds(32 * p, 32), :]

    to_right = [remote(piece(0, p), piece(1, p), xs.at[p], xr.at[p], right) for p in range(3)]
    to_left = [remote(piece(0, p), piece(2, p), xs.at[3 + p], xr.at[3 + p], left) for p in range(3)]
    for k in range(3):
        to_right[k].start()
        to_left[2 - k].start()
    far = [
        remote(piece(1, 0), piece(3, 0), xs.at[6], xr.at[6], right),
        remote(piece(1 + c, 1), piece(3, 1), xs.at[7], xr.at[7], {X: lax.rem(x + 1 + 2 * c, 4)}),
        remote(piece(2, 2), piece(3, 2), xs.at[8], xr.at[8], left),
    ]

    others = pl.ds(1, 3)
    left_columns, right_columns = pl.ds(0, 1024), pl.ds(1024, 1024)
    along_z = [{Z: lax.rem(z + 1, 4)}, {Z: lax.rem(z + 3, 4)}, {Z: lax.rem(z + 1 + 2 * c, 4)}]
    along_y = [{Y: lax.rem(y + 1, 4)}, {Y: lax.rem(y + 3, 4)}, {Y: lax.rem(y + 1 + 2 * c, 4)}]
    passed_z, passed_y = lax.rem(z + 3 + 2 * c, 4), lax.rem(y + 3 + 2 * c, 4)
    every = pl.ds(0, 4)

    def ring(first_src, here, passed, targets, row):
        copies = [remote(first_src, here, ws.at[row, k], wr.at[row, k], targets[k]) for k in range(2)]
        return copies + [remote(passed, passed, ws.at[row, 2], wr.at[row, 2], targets[2])]

    a1 = ring(slice_ref.at[others, :, left_columns], wplane.at[others, z, y, :, left_columns], wplane.at[others, passed_z, y, :, left_columns], along_z, 0)
    b1 = ring(slice_ref.at[others, :, right_columns], wplane.at[others, z, y, :, right_columns], wplane.at[others, z, passed_y, :, right_columns], along_y, 1)
    a2 = ring(wplane.at[others, every, y, :, left_columns], wplane.at[others, every, y, :, left_columns], wplane.at[others, every, passed_y, :, left_columns], along_y, 2)
    b2 = ring(wplane.at[others, z, every, :, right_columns], wplane.at[others, z, every, :, right_columns], wplane.at[others, passed_z, every, :, right_columns], along_z, 3)

    x_ring = [
        remote(wout.at[0, pl.ds(0, 256), :], wout.at[3, pl.ds(0, 256), :], ws.at[4, 0], wr.at[4, 0], right),
        remote(wout.at[0, pl.ds(0, 256), :], wout.at[1, pl.ds(0, 256), :], ws.at[4, 1], wr.at[4, 1], left),
        remote(wout.at[3 - 2 * c, pl.ds(0, 256), :], wout.at[2, pl.ds(0, 256), :], ws.at[4, 2], wr.at[4, 2], {X: lax.rem(x + 1 + 2 * c, 4)}),
    ]

    tri_ref[...] = jnp.where(
        lax.broadcasted_iota(jnp.int32, (KP, KP), 0) >= lax.broadcasted_iota(jnp.int32, (KP, KP), 1), -1.0, 0.0
    ).astype(jnp.bfloat16)
    first = lax.broadcasted_iota(jnp.int32, (96, 96), 0)
    second = lax.broadcasted_iota(jnp.int32, (96, 96), 1)
    shuffle = jnp.where(second == jnp.where(first < 48, 2 * first, 2 * first - 95), 1.0, 0.0).astype(jnp.bfloat16)

    def place(slot):
        return lax.rem(x + (0, 3, 1, 2)[slot], 4)

    def norm_batch(batch, only=(0, 1, 2)):
        gain = norm_gain_ref[...]
        for at, (slot, p) in enumerate(batch):
            if at not in only:
                continue
            for half in range(2):
                rows = xbuf[slot, 32 * p + 16 * half : 32 * p + 16 * half + 16, :].astype(jnp.float32)
                scale = lax.rsqrt(jnp.mean(rows * rows, axis=-1, keepdims=True) + NORM_EPS)
                nbuf[32 * at + 16 * half : 32 * at + 16 * half + 16, :] = (rows * scale * gain).astype(jnp.bfloat16)

    def product(n):
        return jnp.dot(nbuf[...], wbuf[n], preferred_element_type=jnp.float32).astype(jnp.bfloat16)

    def head_norm(rows, gain_ref, factor=1.0):
        rows = rows.astype(jnp.float32)
        return (rows * lax.rsqrt(jnp.mean(rows * rows, axis=-1, keepdims=True) + NORM_EPS) * (gain_ref[...] * factor)).astype(jnp.bfloat16)

    def wait_weights(bt, n):
        if bt == 0:
            weight_copies[n].wait()

    def keys_and_values(bt):
        for half in range(2):
            for kind in range(2):
                wait_weights(bt, 2 * kind + half)
                rows = product(2 * kind + half)
                for i in range(2):
                    part = rows[:, 128 * i : 128 * i + 128]
                    if kind == 0:
                        part = head_norm(part, key_gain_ref)
                    part = jnp.dot(shuffle, part, preferred_element_type=jnp.float32).astype(jnp.bfloat16)
                    skv[bt, 2 * half + i, :, 256 * kind : 256 * kind + 128] = part[:48]
                    skv[bt, 2 * half + i, :, 256 * kind + 128 : 256 * kind + 256] = part[48:]

    def queries(bt):
        for half in range(2):
            wait_weights(bt, 4 + half)
            rows = product(4 + half)
            for i in range(2):
                sq[bt, 2 * half + i] = head_norm(rows[:, 128 * i : 128 * i + 128], query_gain_ref, LOG2E * 128**-0.5)

    def gates(bt):
        for half in range(2):
            wait_weights(bt, 6 + half)
            rows = product(6 + half)
            if bt == 0:
                gate_ref[0, :, 256 * half : 256 * half + 256] = rows
            else:
                sg[bt - 1, :, 256 * half : 256 * half + 256] = rows

    mine = 2 * y + c
    group = {d: 2 * lax.rem(y + d, 4) + c for d in range(4)}
    run_of, runs = {}, []
    for bt in range(4):
        for run in RUNS[bt]:
            run_of.setdefault(bt, []).append(len(runs))
            runs.append((bt, *run))

    def window(r):
        bt, slot, p, at, count = runs[r]
        return pl.ds(pl.multiple_of(48 * place(slot) + 16 * p, 16), 16 * count)

    def query_window(r):
        bt, slot, p, at, count = runs[r]
        return pl.ds(pl.multiple_of(96 * place(slot) + 32 * p, 32), 32 * count)

    def block(r, d):
        return kv_ref.at[:, group[d], window(r), :]

    z_copies, up_copies, down_copies, far_copies, side_copies, q_copies, g_copies = {}, {}, {}, {}, {}, {}, {}
    zig_y = jnp.where(lax.rem(z, 2) == 1, 3 - y, y)
    zig_c = jnp.where(lax.rem(z, 2) == 1, 1 - c, c)
    for r, (bt, slot, p, at, count) in enumerate(runs):
        for d in range(1, 4):
            h = lax.rem(z + d, 4)
            z_copies[r, d] = remote(skv.at[bt, h, pl.ds(16 * at, 16 * count), :], kv_ref.at[z, mine, window(r), :], zs.at[r, d], zr.at[r, d], {Z: h})
        for d in range(4):
            h = lax.rem(z + d, 4)
            target = {Z: h, Y: zig_y, C: zig_c} if d else {Y: 3 - y, C: 1 - c}
            q_copies[r, d] = remote(sq.at[bt, h, pl.ds(32 * at, 32 * count), :], q_ref.at[z, query_window(r), :], qs.at[r, d], qr.at[r, d], target)
        if bt:
            to_rel = (0, 1, 3, 2)[slot]
            g_copies[r] = remote(sg.at[bt - 1, pl.ds(32 * at, 32 * count), :], gate_ref.at[to_rel, pl.ds(32 * p, 32 * count), :], gs.at[r], gr.at[r], {X: place(slot)})
        if bt == 3:
            continue
        up_copies[r] = remote(block(r, 0), block(r, 0), ys.at[r, 0], yr.at[r, 0], up)
        down_copies[r] = remote(block(r, 0), block(r, 0), ys.at[r, 1], yr.at[r, 1], down)
        near = kv_ref.at[:, 2 * lax.rem(y + 3 + 2 * c, 4) + c, window(r), :]
        far_copies[r] = remote(near, near, ys.at[r, 2], yr.at[r, 2], {Y: lax.rem(y + 1 + 2 * c, 4)})
        for d in range(4):
            side_copies[r, d] = remote(block(r, d), block(r, d), ys.at[r, 3 + d], yr.at[r, 3 + d], sibling)

    fine = len(runs) - 1
    fine_up, fine_down, fine_far, fine_side = {}, {}, {}, {}
    for d in range(4):
        source = lax.rem(z + 4 - d, 4)

        def part(place_y):
            return kv_ref.at[source, place_y, window(fine), :]

        fine_up[d] = remote(part(mine), part(mine), fs.at[d, 0], fr.at[d, 0], up)
        fine_down[d] = remote(part(mine), part(mine), fs.at[d, 1], fr.at[d, 1], down)
        near = 2 * lax.rem(y + 3 + 2 * c, 4) + c
        fine_far[d] = remote(part(near), part(near), fs.at[d, 2], fr.at[d, 2], {Y: lax.rem(y + 1 + 2 * c, 4)})
        for k in range(4):
            fine_side[d, k] = remote(part(group[k]), part(group[k]), fs.at[d, 3 + k], fr.at[d, 3 + k], sibling)

    def fine_near(d):
        if d:
            z_copies[fine, d].wait_recv()
        fine_up[d].start()
        fine_down[d].start()
        fine_side[d, 0].start()

    def fine_pass(d):
        fine_up[d].wait_recv()
        fine_down[d].wait_recv()
        fine_far[d].start()
        fine_side[d, 1].start()
        fine_side[d, 3].start()

    def fine_last(d):
        fine_far[d].wait_recv()
        fine_side[d, 2].start()

    def send_z(bt):
        for r in run_of[bt]:
            for d in (2, 1, 3):
                z_copies[r, d].start()
            at, count = runs[r][3], runs[r][4]
            kv_ref[z, mine, window(r), :] = skv[bt, z, 16 * at : 16 * (at + count), :]

    def send_q(bt):
        for r in run_of[bt]:
            at, count = runs[r][3], runs[r][4]
            for d in range(1, 4):
                q_copies[r, d].start()

            @pl.when(lax.rem(z, 2) == 1)
            def _():
                q_copies[r, 0].start()

            @pl.when(lax.rem(z, 2) == 0)
            def _():
                q_ref[z, query_window(r), :] = sq[bt, z, 32 * at : 32 * (at + count), :]

    def send_y(bt):
        for r in run_of[bt]:
            for d in range(1, 4):
                z_copies[r, d].wait_recv()
            up_copies[r].start()
            down_copies[r].start()
            side_copies[r, 0].start()

    def send_far(bt):
        for r in run_of[bt]:
            up_copies[r].wait_recv()
            down_copies[r].wait_recv()
            far_copies[r].start()
            side_copies[r, 1].start()
            side_copies[r, 3].start()

    def send_last(bt):
        for r in run_of[bt]:
            far_copies[r].wait_recv()
            side_copies[r, 2].start()

    def weights_begin():
        for copies in (a1, b1):
            copies[0].start()
            copies[1].start()
        wplane[1:4, z, y] = slice_ref[1:4]

    def weights_pass(first, second):
        for copies in (first, second):
            copies[0].wait_recv()
            copies[1].wait_recv()
            copies[2].start()

    def weights_turn():
        for copies in (a1, b1):
            copies[2].wait_recv()
        for copies in (a2, b2):
            copies[0].start()
            copies[1].start()

    def weights_pass_x():
        for copy in x_ring[:2]:
            copy.wait_recv()
        x_ring[2].start()


    norm_batch(BATCHES[0])
    keys_and_values(0)
    send_z(0)
    queries(0)
    gates(0)
    to_right[0].wait_recv()
    far[0].start()
    to_left[2].wait_recv()
    far[2].start()
    send_y(0)
    to_right[1].wait_recv()
    to_left[1].wait_recv()
    far[1].start()
    own_copies = [pltpu.make_async_copy(wo_ref.at[pl.ds(0, 256), half_columns], wout.at[0, pl.ds(0, 256), :], out_sem.at[16])]
    own_copies += [
        pltpu.make_async_copy(wo_ref.at[pl.ds(256 + 16 * p, 16), half_columns], wplane.at[0, p // 4, p % 4], out_sem.at[p])
        for p in range(16)
    ]
    for copy in own_copies:
        copy.start()
    slice_copy = pltpu.make_async_copy(
        wo_ref.at[pl.ds(pl.multiple_of(256 + 64 * z + 16 * y, 16), 16), half_columns],
        slice_ref.at[0], local_sem.at[9])
    slice_copy.start()
    norm_batch(BATCHES[1])
    keys_and_values(1)
    send_z(1)
    send_far(0)
    send_q(0)
    queries(1)
    send_q(1)
    gates(1)
    send_y(1)
    to_right[2].wait_recv()
    to_left[0].wait_recv()
    norm_batch(BATCHES[2])
    keys_and_values(2)
    send_z(2)
    send_far(1)
    send_last(0)
    queries(2)
    send_q(2)
    gates(2)
    send_y(2)
    for k in (0, 2, 1):
        far[k].wait_recv()
        norm_batch(BATCHES[3], (k,))
    slice_copy.wait()
    slice_copies = [remote(slice_ref.at[0], slice_ref.at[(4 - d) % 4], xs.at[8 + d], xr.at[8 + d], {X: lax.rem(x + d, 4)}) for d in range(1, 4)]
    for copy in slice_copies:
        copy.start()
    for copy in own_copies:
        copy.wait()
    for copy in x_ring[:2]:
        copy.start()
    keys_and_values(3)
    send_z(3)
    fine_near(0)
    send_last(1)
    queries(3)
    send_q(3)
    fine_near(1)
    fine_near(3)
    send_far(2)
    fine_near(2)
    fine_pass(0)
    gates(3)
    fine_pass(1)
    fine_pass(3)
    fine_pass(2)
    for copy in slice_copies:
        copy.wait_recv()
    weights_begin()
    send_last(2)
    for d in (0, 1, 3, 2):
        fine_last(d)
    for r in range(len(runs)):
        if runs[r][0]:
            g_copies[r].start()
    for r in range(len(runs)):
        for d in range(4):
            (side_copies[r, d] if r != fine else fine_side[d, 0]).wait_recv()
        for d in range(1, 4):
            q_copies[r, d].wait_recv()

        @pl.when(lax.rem(z, 2) == 1)
        def _():
            q_copies[r, 0].wait_recv()

    for d in range(4):
        for k in range(1, 4):
            fine_side[d, k].wait_recv()
    off = off_ref[z] * LOG2E
    kv_rows = kv_ref.reshape(6144, 512)

    def keys_of(kind, start):
        return kv_rows[pl.ds(start, KP), 128 * kind : 128 * kind + 128]


    dn = (((1,), (1,)), ((), ()))

    def score(i, b, k, slot, masked):
        start = pl.multiple_of(jnp.maximum(k, 0) * KP, KP)
        q = q_ref[i]
        ea = jnp.exp2(lax.dot_general(q, keys_of(0, start), dn, preferred_element_type=jnp.float32) + off)
        eb = jnp.exp2(lax.dot_general(q, keys_of(1, start), dn, preferred_element_type=jnp.float32) + off)
        if masked:
            row = lax.broadcasted_iota(jnp.int32, (NQ, KP), 0) + b * NQ
            col = lax.broadcasted_iota(jnp.int32, (NQ, KP), 1) * 2 + k * KS
            ea = jnp.where((col < row) & (col >= 0), ea, 0.0)
            eb = jnp.where((col + 1 < row) & (col >= 0), eb, 0.0)
        ta = 1.0 + ea
        lbuf[slot] = jnp.log2(ta * (1.0 + eb)).astype(jnp.bfloat16)
        abuf[slot] = ea
        bbuf[slot] = eb * ta

    def gather(k, slot):
        start = pl.multiple_of(jnp.maximum(k, 0) * KP, KP)
        s = jnp.dot(lbuf[slot], tri_ref[...], preferred_element_type=jnp.float32)
        g = jnp.exp2(s)
        wa = (abuf[slot] * g).astype(jnp.bfloat16)
        wb = (bbuf[slot] * g).astype(jnp.bfloat16)
        part = jnp.dot(wa, keys_of(2, start), preferred_element_type=jnp.float32)
        part += jnp.dot(wb, keys_of(3, start), preferred_element_type=jnp.float32)
        carry = carry_ref[...]
        acc_ref[...] += part * jnp.exp2(carry)
        carry_ref[...] = carry + jnp.broadcast_to(s[:, 0:1], (NQ, 128))

    def two_steps(i, b, k, masked):
        score(i, b, k, 0, masked)
        score(i, b, k - 1, 1, masked)
        gather(k, 0)
        gather(k - 1, 1)

    def steps(i, b, top, count):
        def pair(t, unused):
            two_steps(i, b, top - 2 * t, False)
            return unused

        def last(t, unused):
            score(i, b, top - count + 1, 0, False)
            gather(top - count + 1, 0)
            return unused

        lax.fori_loop(0, count // 2, pair, 0)
        lax.fori_loop(0, lax.rem(count, 2), last, 0)

    def sends(i):
        target = {Y: 3 - y, C: 1 - c} if i % 2 else {}
        out = []
        for rel in range(4):
            there = lax.rem(x + 4 - rel, 4)
            out.append(remote(sa.at[i, pl.ds(pl.multiple_of(96 * there, 32), 96), :], att.at[rel, z], as_.at[i, rel], ar.at[z, rel], {Z: i, X: there, **target}))
        return out

    def unless_own(i, rel, work):
        if rel or i % 2:
            work()
        else:
            pl.when(z != i)(work)

    for i in (3, 2, 1, 0):
        b = 8 * i + (7 - mine if i % 2 else mine)
        acc_ref[...] = jnp.zeros_like(acc_ref)
        carry_ref[...] = jnp.zeros_like(carry_ref)
        n_hi = (b * NQ + NQ + KS - 1) // KS
        two_steps(i, b, n_hi - 1, True)
        if i == 3:
            weights_pass(a1, b1)
            steps(i, b, n_hi - 3, 6)
            weights_turn()
            steps(i, b, n_hi - 9, 6)
            weights_pass_x()
            steps(i, b, n_hi - 15, n_hi - 14)
        elif i == 2:
            steps(i, b, n_hi - 3, 8)
            weights_pass(a2, b2)
            steps(i, b, n_hi - 11, n_hi - 10)
        else:
            steps(i, b, n_hi - 3, jnp.maximum(n_hi - 2, 0))
        total = acc_ref[...]
        scale = lax.rsqrt(jnp.mean(total * total, axis=-1, keepdims=True) + NORM_EPS)
        sa[i] = (total * scale * gain_ref[z]).astype(jnp.bfloat16)
        for rel, copy in enumerate(sends(i)):
            unless_own(i, rel, copy.start)
        if i % 2 == 0:
            @pl.when(z == i)
            def _():
                att[0, z] = sa[i, pl.ds(pl.multiple_of(96 * x, 32), 96), :]

    for r in range(len(runs)):
        if runs[r][0]:
            g_copies[r].wait_recv()
    to_sibling = [remote(mx.at[0, :, pl.ds(512 * r, 512)], mx.at[1, :, pl.ds(512 * r, 512)], ms.at[r], mr.at[r], sibling) for r in range(4)]
    for r in range(4):
        for h in range(4):
            here = att.at[r, h]
            unless_own(h, r, remote(here, here, as_.at[h, r], ar.at[h, r], sibling).wait_recv)
        for h in range(4):
            gate = gate_ref[r, :, 128 * h : 128 * h + 128].astype(jnp.float32)
            mixed = att[r, h].astype(jnp.float32) * (gate / (1.0 + jnp.exp(-gate)))
            mx[0, :, 512 * r + 128 * h : 512 * r + 128 * h + 128] = mixed.astype(jnp.bfloat16)
        to_sibling[r].start()
    for copies in (a2, b2):
        copies[2].wait_recv()
    x_ring[2].wait_recv()
    for copy in to_sibling:
        copy.wait_recv()
    backs = []
    rows = mx[...].reshape(192, 2048)
    for n in range(8):
        total = jnp.zeros((192, 256), jnp.float32)
        for r in range(4):
            near = wout[r, :, 256 * n : 256 * n + 256]
            spread = wplane[r, :, :, :, 256 * n : 256 * n + 256].reshape(256, 256)
            total += jnp.dot(rows[:, 512 * r : 512 * r + 256], near, preferred_element_type=jnp.float32)
            total += jnp.dot(rows[:, 512 * r + 256 : 512 * r + 512], spread, preferred_element_type=jnp.float32)
        total = total.astype(jnp.bfloat16)
        columns = pl.ds(pl.multiple_of(2048 * c + 256 * n, 256), 256)
        so[n] = total[96:]
        back = remote(so.at[n], out_ref.at[:, columns], ms.at[4 + n], mr.at[4 + n], sibling)
        back.start()
        backs.append(back)
        out_ref[:, columns] = total[:96]
    for back in backs:
        back.wait()
    for copy in to_sibling:
        copy.wait_send()
    for i in range(4):
        for rel, copy in enumerate(sends(i)):
            unless_own(i, rel, copy.wait_send)
    for copies in (a1, b1, a2, b2, x_ring):
        for copy in copies:
            copy.wait_send()
    for r in range(len(runs)):
        @pl.when(lax.rem(z, 2) == 1)
        def _():
            q_copies[r, 0].wait_send()

        for d in range(1, 4):
            z_copies[r, d].wait_send()
            q_copies[r, d].wait_send()
        if r != fine:
            for d in range(4):
                side_copies[r, d].wait_send()
            up_copies[r].wait_send()
            down_copies[r].wait_send()
            far_copies[r].wait_send()
        if runs[r][0]:
            g_copies[r].wait_send()
    for d in range(4):
        for copy in (fine_up[d], fine_down[d], fine_far[d], *(fine_side[d, k] for k in range(4))):
            copy.wait_send()
    for copy in slice_copies + to_right + to_left + far:
        copy.wait_send()


def layer(tokens, norm_gain, query_gain, key_gain, wq, wk, wv, wg, wo, offset, gain):
    vm = pl.BlockSpec(memory_space=pltpu.VMEM)
    hbm = pl.BlockSpec(memory_space=pltpu.HBM)
    smem = pl.BlockSpec(memory_space=pltpu.SMEM)
    count = sum(len(run) for run in RUNS)
    sems = pltpu.SemaphoreType.DMA
    half, full = jnp.bfloat16, jnp.float32
    return pl.pallas_call(
        layer_kernel,
        out_shape=jax.ShapeDtypeStruct((96, 4096), jnp.bfloat16),
        in_specs=[hbm, vm, vm, vm, hbm, hbm, hbm, hbm, hbm, vm, smem],
        out_specs=vm,
        scratch_shapes=[
            pltpu.VMEM((4, 8, 192, 512), half),
            pltpu.VMEM((4, NQ, 128), half),
            pltpu.VMEM((4, 96, 512), half),
            pltpu.VMEM((4, 16, 2048), half),
            pltpu.VMEM((4, 256, 2048), half),
            pltpu.VMEM((4, 4, 4, 16, 2048), half),
            pltpu.VMEM((4, 4, 96, 128), half),
            pltpu.VMEM((4, NQ, 128), half),
            pltpu.VMEM((2, 96, 2048), half),
            pltpu.VMEM((8, 96, 256), half),
            pltpu.VMEM((NQ, 128), full),
            pltpu.VMEM((NQ, 128), full),
            pltpu.VMEM((2, NQ, KP), half),
            pltpu.VMEM((2, NQ, KP), full),
            pltpu.VMEM((2, NQ, KP), full),
            pltpu.VMEM((KP, KP), half),
            pltpu.VMEM((4, 96, 4096), half),
            pltpu.VMEM((96, 4096), half),
            pltpu.VMEM((8, 4096, 256), half),
            pltpu.VMEM((4, 4, 48, 512), half),
            pltpu.VMEM((4, 4, 96, 128), half),
            pltpu.VMEM((3, 96, 512), half),
            sems((10,)), sems((12,)), sems((12,)),
            sems((count, 4)), sems((count, 4)),
            sems((count, 7)), sems((count, 7)),
            sems((count, 4)), sems((count, 4)),
            sems((count,)), sems((count,)),
            sems((4, 7)), sems((4, 7)),
            sems((17,)), sems((5, 3)), sems((5, 3)),
            sems((4, 4)), sems((4, 4)), sems((12,)), sems((12,)),
        ],
        compiler_params=pltpu.CompilerParams(collective_id=0, has_side_effects=True, vmem_limit_bytes=56 * 2**20),
    )(tokens, norm_gain.reshape(1, -1), query_gain.reshape(1, -1), key_gain.reshape(1, -1), wq, wk, wv, wg, wo, gain.reshape(4, 1, 128), offset)


def on_device(tokens, norm_gain, query_weight, key_weight, value_weight, gate_weight, query_gain, key_gain, score_offset, out_gain, out_weight):
    return layer(tokens, norm_gain, query_gain, key_gain, query_weight, key_weight, value_weight, gate_weight, out_weight, score_offset, out_gain)


def solution(mesh):
    finer = Mesh(mesh.devices.reshape(4, 4, 2, mesh.shape["tp"]), ("sp_0", "sp_1", "sp_2", "tp"))
    in_specs = (P(SP_TP, None), P(), P(None, "tp"), P(None, "tp"), P(None, "tp"), P(None, "tp"), P(), P(), P("tp"), P("tp"), P("tp", None))
    return jax.shard_map(on_device, mesh=finer, in_specs=in_specs, out_specs=P(SP_TP, None), check_vma=False)
```

```python
import functools

import jax
import jax.numpy as jnp
from jax import lax
from jax.experimental import pallas as pl
from jax.experimental.pallas import tpu as pltpu
from jax.sharding import Mesh
from jax.sharding import PartitionSpec as P

SP_TP = ("sp_0", "sp_1", "sp_2", "tp")
NORM_EPS = 1e-06
NQ = 384
KS = 512
KP = 256
LOG2E = 1.4426950408889634

MESH = pl.DeviceIdType.MESH
X, Y, Z, C = "tp", "sp_1", "sp_0", "sp_2"
BATCHES = (
    ((0, 0), (0, 1), (0, 2)),
    ((1, 0), (1, 1), (2, 2)),
    ((1, 2), (2, 0), (2, 1)),
    ((3, 0), (3, 1), (3, 2)),
)


def pieces_in_runs(batch):
    runs = []
    for at, (slot, piece) in enumerate(batch):
        if runs and runs[-1][0] == slot and runs[-1][1] + runs[-1][3] == piece:
            runs[-1][3] += 1
        else:
            runs.append([slot, piece, at, 1])
    return runs


RUNS = [pieces_in_runs(batch) for batch in BATCHES]


def layer_kernel(tokens_ref, norm_gain_ref, query_gain_ref, key_gain_ref, wq_ref, wk_ref, wv_ref, wg_ref, wo_ref,
                      gain_ref, off_ref, out_ref,
                      kv_ref, q_ref, gate_ref, slice_ref, wout, wplane, att, sa, mx, so, acc_ref, carry_ref, lbuf, fbuf, abuf, bbuf, tri_ref,
                      xbuf, nbuf, wbuf, skv, sq, sg, local_sem, xs, xr, zs, zr, ys, yr, qs, qr, gs, gr, fs, fr,
                      out_sem, ws, wr, as_, ar, ms, mr):
    x, y, z, c = (lax.axis_index(name) for name in (X, Y, Z, C))
    half_columns = pl.ds(pl.multiple_of(2048 * c, 2048), 2048)
    token_copy = pltpu.make_async_copy(tokens_ref, xbuf.at[0], local_sem.at[8])
    token_copy.start()
    right, left = {X: lax.rem(x + 1, 4)}, {X: lax.rem(x + 3, 4)}
    up, down = {Y: lax.rem(y + 1, 4)}, {Y: lax.rem(y + 3, 4)}
    sibling = {C: 1 - c}
    barrier = pltpu.get_barrier_semaphore()
    partners = [right, left, up, down, sibling]
    partners += [{Z: lax.rem(z + d, 4)} for d in range(1, 4)]
    for partner in partners:
        pl.semaphore_signal(barrier, inc=1, device_id=partner, device_id_type=MESH)
    token_copy.wait()
    weight_copies = []
    for kind, ref in enumerate((wk_ref, wv_ref, wq_ref, wg_ref)):
        for half in range(2):
            weight_copies.append(pltpu.make_async_copy(ref.at[:, pl.ds(256 * half, 256)], wbuf.at[2 * kind + half], local_sem.at[2 * kind + half]))
    for copy in weight_copies:
        copy.start()
    pl.semaphore_wait(barrier, len(partners))

    def remote(src, dst, send, recv, target):
        return pltpu.make_async_remote_copy(src_ref=src, dst_ref=dst, send_sem=send, recv_sem=recv, device_id=target, device_id_type=MESH)

    def piece(slot, p):
        return xbuf.at[slot, pl.ds(32 * p, 32), :]

    to_right = [remote(piece(0, p), piece(1, p), xs.at[p], xr.at[p], right) for p in range(3)]
    to_left = [remote(piece(0, p), piece(2, p), xs.at[3 + p], xr.at[3 + p], left) for p in range(3)]
    for k in range(3):
        to_right[k].start()
        to_left[2 - k].start()
    far = [
        remote(piece(1, 0), piece(3, 0), xs.at[6], xr.at[6], right),
        remote(piece(1 + c, 1), piece(3, 1), xs.at[7], xr.at[7], {X: lax.rem(x + 1 + 2 * c, 4)}),
        remote(piece(2, 2), piece(3, 2), xs.at[8], xr.at[8], left),
    ]

    others = pl.ds(1, 3)
    left_columns, right_columns = pl.ds(0, 1024), pl.ds(1024, 1024)
    along_z = [{Z: lax.rem(z + 1, 4)}, {Z: lax.rem(z + 3, 4)}, {Z: lax.rem(z + 1 + 2 * c, 4)}]
    along_y = [{Y: lax.rem(y + 1, 4)}, {Y: lax.rem(y + 3, 4)}, {Y: lax.rem(y + 1 + 2 * c, 4)}]
    passed_z, passed_y = lax.rem(z + 3 + 2 * c, 4), lax.rem(y + 3 + 2 * c, 4)
    every = pl.ds(0, 4)

    def ring(first_src, here, passed, targets, row):
        copies = [remote(first_src, here, ws.at[row, k], wr.at[row, k], targets[k]) for k in range(2)]
        return copies + [remote(passed, passed, ws.at[row, 2], wr.at[row, 2], targets[2])]

    a1 = ring(slice_ref.at[others, :, left_columns], wplane.at[others, z, y, :, left_columns], wplane.at[others, passed_z, y, :, left_columns], along_z, 0)
    b1 = ring(slice_ref.at[others, :, right_columns], wplane.at[others, z, y, :, right_columns], wplane.at[others, z, passed_y, :, right_columns], along_y, 1)
    a2 = ring(wplane.at[others, every, y, :, left_columns], wplane.at[others, every, y, :, left_columns], wplane.at[others, every, passed_y, :, left_columns], along_y, 2)
    b2 = ring(wplane.at[others, z, every, :, right_columns], wplane.at[others, z, every, :, right_columns], wplane.at[others, passed_z, every, :, right_columns], along_z, 3)

    x_ring = [
        remote(wout.at[0, pl.ds(0, 256), :], wout.at[3, pl.ds(0, 256), :], ws.at[4, 0], wr.at[4, 0], right),
        remote(wout.at[0, pl.ds(0, 256), :], wout.at[1, pl.ds(0, 256), :], ws.at[4, 1], wr.at[4, 1], left),
        remote(wout.at[3 - 2 * c, pl.ds(0, 256), :], wout.at[2, pl.ds(0, 256), :], ws.at[4, 2], wr.at[4, 2], {X: lax.rem(x + 1 + 2 * c, 4)}),
    ]

    tri_ref[...] = jnp.where(
        lax.broadcasted_iota(jnp.int32, (KP, KP), 0) > lax.broadcasted_iota(jnp.int32, (KP, KP), 1), -1.0, 0.0
    ).astype(jnp.bfloat16)
    first = lax.broadcasted_iota(jnp.int32, (96, 96), 0)
    second = lax.broadcasted_iota(jnp.int32, (96, 96), 1)
    shuffle = jnp.where(second == jnp.where(first < 48, 2 * first, 2 * first - 95), 1.0, 0.0).astype(jnp.bfloat16)

    def place(slot):
        return lax.rem(x + (0, 3, 1, 2)[slot], 4)

    def norm_batch(batch, only=(0, 1, 2)):
        gain = norm_gain_ref[...]
        for at, (slot, p) in enumerate(batch):
            if at not in only:
                continue
            for half in range(2):
                rows = xbuf[slot, 32 * p + 16 * half : 32 * p + 16 * half + 16, :].astype(jnp.float32)
                scale = lax.rsqrt(jnp.mean(rows * rows, axis=-1, keepdims=True) + NORM_EPS)
                nbuf[32 * at + 16 * half : 32 * at + 16 * half + 16, :] = (rows * scale * gain).astype(jnp.bfloat16)

    def product(n):
        return jnp.dot(nbuf[...], wbuf[n], preferred_element_type=jnp.float32).astype(jnp.bfloat16)

    def head_norm(rows, gain_ref, factor=1.0):
        rows = rows.astype(jnp.float32)
        return (rows * lax.rsqrt(jnp.mean(rows * rows, axis=-1, keepdims=True) + NORM_EPS) * (gain_ref[...] * factor)).astype(jnp.bfloat16)

    def wait_weights(bt, n):
        if bt == 0:
            weight_copies[n].wait()

    def keys_and_values(bt):
        for half in range(2):
            for kind in range(2):
                wait_weights(bt, 2 * kind + half)
                rows = product(2 * kind + half)
                for i in range(2):
                    part = rows[:, 128 * i : 128 * i + 128]
                    if kind == 0:
                        part = head_norm(part, key_gain_ref)
                    part = jnp.dot(shuffle, part, preferred_element_type=jnp.float32).astype(jnp.bfloat16)
                    skv[bt, 2 * half + i, :, 256 * kind : 256 * kind + 128] = part[:48]
                    skv[bt, 2 * half + i, :, 256 * kind + 128 : 256 * kind + 256] = part[48:]

    def queries(bt):
        for half in range(2):
            wait_weights(bt, 4 + half)
            rows = product(4 + half)
            for i in range(2):
                sq[bt, 2 * half + i] = head_norm(rows[:, 128 * i : 128 * i + 128], query_gain_ref, LOG2E * 128**-0.5)

    def gates(bt):
        for half in range(2):
            wait_weights(bt, 6 + half)
            rows = product(6 + half)
            if bt == 0:
                gate_ref[0, :, 256 * half : 256 * half + 256] = rows
            else:
                sg[bt - 1, :, 256 * half : 256 * half + 256] = rows

    mine = 2 * y + c
    group = {d: 2 * lax.rem(y + d, 4) + c for d in range(4)}
    run_of, runs = {}, []
    for bt in range(4):
        for run in RUNS[bt]:
            run_of.setdefault(bt, []).append(len(runs))
            runs.append((bt, *run))

    def window(r):
        bt, slot, p, at, count = runs[r]
        return pl.ds(pl.multiple_of(48 * place(slot) + 16 * p, 16), 16 * count)

    def query_window(r):
        bt, slot, p, at, count = runs[r]
        return pl.ds(pl.multiple_of(96 * place(slot) + 32 * p, 32), 32 * count)

    def block(r, d):
        return kv_ref.at[:, group[d], window(r), :]

    z_copies, up_copies, down_copies, far_copies, side_copies, q_copies, g_copies = {}, {}, {}, {}, {}, {}, {}
    zig_y = jnp.where(lax.rem(z, 2) == 1, 3 - y, y)
    zig_c = jnp.where(lax.rem(z, 2) == 1, 1 - c, c)
    for r, (bt, slot, p, at, count) in enumerate(runs):
        for d in range(1, 4):
            h = lax.rem(z + d, 4)
            z_copies[r, d] = remote(skv.at[bt, h, pl.ds(16 * at, 16 * count), :], kv_ref.at[z, mine, window(r), :], zs.at[r, d], zr.at[r, d], {Z: h})
        for d in range(4):
            h = lax.rem(z + d, 4)
            target = {Z: h, Y: zig_y, C: zig_c} if d else {Y: 3 - y, C: 1 - c}
            q_copies[r, d] = remote(sq.at[bt, h, pl.ds(32 * at, 32 * count), :], q_ref.at[z, query_window(r), :], qs.at[r, d], qr.at[r, d], target)
        if bt:
            to_rel = (0, 1, 3, 2)[slot]
            g_copies[r] = remote(sg.at[bt - 1, pl.ds(32 * at, 32 * count), :], gate_ref.at[to_rel, pl.ds(32 * p, 32 * count), :], gs.at[r], gr.at[r], {X: place(slot)})
        if bt == 3:
            continue
        up_copies[r] = remote(block(r, 0), block(r, 0), ys.at[r, 0], yr.at[r, 0], up)
        down_copies[r] = remote(block(r, 0), block(r, 0), ys.at[r, 1], yr.at[r, 1], down)
        near = kv_ref.at[:, 2 * lax.rem(y + 3 + 2 * c, 4) + c, window(r), :]
        far_copies[r] = remote(near, near, ys.at[r, 2], yr.at[r, 2], {Y: lax.rem(y + 1 + 2 * c, 4)})
        for d in range(4):
            side_copies[r, d] = remote(block(r, d), block(r, d), ys.at[r, 3 + d], yr.at[r, 3 + d], sibling)

    fine = len(runs) - 1
    fine_up, fine_down, fine_far, fine_side = {}, {}, {}, {}
    for d in range(4):
        source = lax.rem(z + 4 - d, 4)

        def part(place_y):
            return kv_ref.at[source, place_y, window(fine), :]

        fine_up[d] = remote(part(mine), part(mine), fs.at[d, 0], fr.at[d, 0], up)
        fine_down[d] = remote(part(mine), part(mine), fs.at[d, 1], fr.at[d, 1], down)
        near = 2 * lax.rem(y + 3 + 2 * c, 4) + c
        fine_far[d] = remote(part(near), part(near), fs.at[d, 2], fr.at[d, 2], {Y: lax.rem(y + 1 + 2 * c, 4)})
        for k in range(4):
            fine_side[d, k] = remote(part(group[k]), part(group[k]), fs.at[d, 3 + k], fr.at[d, 3 + k], sibling)

    def fine_near(d):
        if d:
            z_copies[fine, d].wait_recv()
        fine_up[d].start()
        fine_down[d].start()
        fine_side[d, 0].start()

    def fine_pass(d):
        fine_up[d].wait_recv()
        fine_down[d].wait_recv()
        fine_far[d].start()
        fine_side[d, 1].start()
        fine_side[d, 3].start()

    def fine_last(d):
        fine_far[d].wait_recv()
        fine_side[d, 2].start()

    def send_z(bt):
        for r in run_of[bt]:
            for d in (2, 1, 3):
                z_copies[r, d].start()
            at, count = runs[r][3], runs[r][4]
            kv_ref[z, mine, window(r), :] = skv[bt, z, 16 * at : 16 * (at + count), :]

    def send_q(bt):
        for r in run_of[bt]:
            at, count = runs[r][3], runs[r][4]
            for d in range(1, 4):
                q_copies[r, d].start()

            @pl.when(lax.rem(z, 2) == 1)
            def _():
                q_copies[r, 0].start()

            @pl.when(lax.rem(z, 2) == 0)
            def _():
                q_ref[z, query_window(r), :] = sq[bt, z, 32 * at : 32 * (at + count), :]

    def send_y(bt):
        for r in run_of[bt]:
            for d in range(1, 4):
                z_copies[r, d].wait_recv()
            up_copies[r].start()
            down_copies[r].start()
            side_copies[r, 0].start()

    def send_far(bt):
        for r in run_of[bt]:
            up_copies[r].wait_recv()
            down_copies[r].wait_recv()
            far_copies[r].start()
            side_copies[r, 1].start()
            side_copies[r, 3].start()

    def send_last(bt):
        for r in run_of[bt]:
            far_copies[r].wait_recv()
            side_copies[r, 2].start()

    def weights_begin():
        for copies in (a1, b1):
            copies[0].start()
            copies[1].start()
        wplane[1:4, z, y] = slice_ref[1:4]

    def weights_pass(first, second):
        for copies in (first, second):
            copies[0].wait_recv()
            copies[1].wait_recv()
            copies[2].start()

    def weights_turn():
        for copies in (a1, b1):
            copies[2].wait_recv()
        for copies in (a2, b2):
            copies[0].start()
            copies[1].start()

    def weights_pass_x():
        for copy in x_ring[:2]:
            copy.wait_recv()
        x_ring[2].start()


    norm_batch(BATCHES[0])
    keys_and_values(0)
    send_z(0)
    queries(0)
    gates(0)
    to_right[0].wait_recv()
    far[0].start()
    to_left[2].wait_recv()
    far[2].start()
    send_y(0)
    to_right[1].wait_recv()
    to_left[1].wait_recv()
    far[1].start()
    own_copies = [pltpu.make_async_copy(wo_ref.at[pl.ds(0, 256), half_columns], wout.at[0, pl.ds(0, 256), :], out_sem.at[16])]
    own_copies += [
        pltpu.make_async_copy(wo_ref.at[pl.ds(256 + 16 * p, 16), half_columns], wplane.at[0, p // 4, p % 4], out_sem.at[p])
        for p in range(16)
    ]
    for copy in own_copies:
        copy.start()
    slice_copy = pltpu.make_async_copy(
        wo_ref.at[pl.ds(pl.multiple_of(256 + 64 * z + 16 * y, 16), 16), half_columns],
        slice_ref.at[0], local_sem.at[9])
    slice_copy.start()
    norm_batch(BATCHES[1])
    keys_and_values(1)
    send_z(1)
    send_far(0)
    send_q(0)
    queries(1)
    send_q(1)
    gates(1)
    send_y(1)
    to_right[2].wait_recv()
    to_left[0].wait_recv()
    norm_batch(BATCHES[2])
    keys_and_values(2)
    send_z(2)
    send_far(1)
    send_last(0)
    queries(2)
    send_q(2)
    gates(2)
    send_y(2)
    for k in (0, 2, 1):
        far[k].wait_recv()
        norm_batch(BATCHES[3], (k,))
    slice_copy.wait()
    slice_copies = [remote(slice_ref.at[0], slice_ref.at[(4 - d) % 4], xs.at[8 + d], xr.at[8 + d], {X: lax.rem(x + d, 4)}) for d in range(1, 4)]
    for copy in slice_copies:
        copy.start()
    for copy in own_copies:
        copy.wait()
    for copy in x_ring[:2]:
        copy.start()
    keys_and_values(3)
    send_z(3)
    fine_near(0)
    send_last(1)
    queries(3)
    send_q(3)
    fine_near(1)
    fine_near(3)
    send_far(2)
    fine_near(2)
    fine_pass(0)
    gates(3)
    fine_pass(1)
    fine_pass(3)
    fine_pass(2)
    for copy in slice_copies:
        copy.wait_recv()
    weights_begin()
    send_last(2)
    for d in (0, 1, 3, 2):
        fine_last(d)
    for r in range(len(runs)):
        if runs[r][0]:
            g_copies[r].start()
    for r in range(len(runs)):
        for d in range(4):
            (side_copies[r, d] if r != fine else fine_side[d, 0]).wait_recv()
        for d in range(1, 4):
            q_copies[r, d].wait_recv()

        @pl.when(lax.rem(z, 2) == 1)
        def _():
            q_copies[r, 0].wait_recv()

    for d in range(4):
        for k in range(1, 4):
            fine_side[d, k].wait_recv()
    off = off_ref[z] * LOG2E
    kv_rows = kv_ref.reshape(6144, 512)

    def keys_of(kind, start):
        return kv_rows[pl.ds(start, KP), 128 * kind : 128 * kind + 128]


    dn = (((1,), (1,)), ((), ()))

    def score(i, b, k, slot, masked):
        start = pl.multiple_of(jnp.maximum(k, 0) * KP, KP)
        q = q_ref[i]
        ea = jnp.exp2(lax.dot_general(q, keys_of(0, start), dn, preferred_element_type=jnp.float32) + off)
        eb = jnp.exp2(lax.dot_general(q, keys_of(1, start), dn, preferred_element_type=jnp.float32) + off)
        if masked:
            row = lax.broadcasted_iota(jnp.int32, (NQ, KP), 0) + b * NQ
            col = lax.broadcasted_iota(jnp.int32, (NQ, KP), 1) * 2 + k * KS
            ea = jnp.where((col < row) & (col >= 0), ea, 0.0)
            eb = jnp.where((col + 1 < row) & (col >= 0), eb, 0.0)
        ta = 1.0 + ea
        logs = jnp.log2(ta * (1.0 + eb))
        lbuf[slot] = logs.astype(jnp.bfloat16)
        fbuf[slot] = logs
        abuf[slot] = ea
        bbuf[slot] = eb * ta

    def gather(k, slot):
        start = pl.multiple_of(jnp.maximum(k, 0) * KP, KP)
        s = jnp.dot(lbuf[slot], tri_ref[...], preferred_element_type=jnp.float32) - fbuf[slot]
        g = jnp.exp2(s)
        wa = (abuf[slot] * g).astype(jnp.bfloat16)
        wb = (bbuf[slot] * g).astype(jnp.bfloat16)
        part = jnp.dot(wa, keys_of(2, start), preferred_element_type=jnp.float32)
        part += jnp.dot(wb, keys_of(3, start), preferred_element_type=jnp.float32)
        carry = carry_ref[...]
        acc_ref[...] += part * jnp.exp2(carry)
        carry_ref[...] = carry + jnp.broadcast_to(s[:, 0:1], (NQ, 128))

    def two_steps(i, b, k, masked):
        score(i, b, k, 0, masked)
        score(i, b, k - 1, 1, masked)
        gather(k, 0)
        gather(k - 1, 1)

    def steps(i, b, top, count):
        def pair(t, unused):
            two_steps(i, b, top - 2 * t, False)
            return unused

        def last(t, unused):
            score(i, b, top - count + 1, 0, False)
            gather(top - count + 1, 0)
            return unused

        lax.fori_loop(0, count // 2, pair, 0)
        lax.fori_loop(0, lax.rem(count, 2), last, 0)

    def sends(i):
        target = {Y: 3 - y, C: 1 - c} if i % 2 else {}
        out = []
        for rel in range(4):
            there = lax.rem(x + 4 - rel, 4)
            out.append(remote(sa.at[i, pl.ds(pl.multiple_of(96 * there, 32), 96), :], att.at[rel, z], as_.at[i, rel], ar.at[z, rel], {Z: i, X: there, **target}))
        return out

    def unless_own(i, rel, work):
        if rel or i % 2:
            work()
        else:
            pl.when(z != i)(work)

    for i in (3, 2, 1, 0):
        b = 8 * i + (7 - mine if i % 2 else mine)
        acc_ref[...] = jnp.zeros_like(acc_ref)
        carry_ref[...] = jnp.zeros_like(carry_ref)
        n_hi = (b * NQ + NQ + KS - 1) // KS
        two_steps(i, b, n_hi - 1, True)
        if i == 3:
            weights_pass(a1, b1)
            steps(i, b, n_hi - 3, 6)
            weights_turn()
            steps(i, b, n_hi - 9, 6)
            weights_pass_x()
            steps(i, b, n_hi - 15, n_hi - 14)
        elif i == 2:
            steps(i, b, n_hi - 3, 8)
            weights_pass(a2, b2)
            steps(i, b, n_hi - 11, n_hi - 10)
        else:
            steps(i, b, n_hi - 3, jnp.maximum(n_hi - 2, 0))
        total = acc_ref[...]
        scale = lax.rsqrt(jnp.mean(total * total, axis=-1, keepdims=True) + NORM_EPS)
        sa[i] = (total * scale * gain_ref[z]).astype(jnp.bfloat16)
        for rel, copy in enumerate(sends(i)):
            unless_own(i, rel, copy.start)
        if i % 2 == 0:
            @pl.when(z == i)
            def _():
                att[0, z] = sa[i, pl.ds(pl.multiple_of(96 * x, 32), 96), :]

    for r in range(len(runs)):
        if runs[r][0]:
            g_copies[r].wait_recv()
    to_sibling = [remote(mx.at[0, :, pl.ds(512 * r, 512)], mx.at[1, :, pl.ds(512 * r, 512)], ms.at[r], mr.at[r], sibling) for r in range(4)]
    for r in range(4):
        for h in range(4):
            here = att.at[r, h]
            unless_own(h, r, remote(here, here, as_.at[h, r], ar.at[h, r], sibling).wait_recv)
        for h in range(4):
            gate = gate_ref[r, :, 128 * h : 128 * h + 128].astype(jnp.float32)
            mixed = att[r, h].astype(jnp.float32) * (gate / (1.0 + jnp.exp(-gate)))
            mx[0, :, 512 * r + 128 * h : 512 * r + 128 * h + 128] = mixed.astype(jnp.bfloat16)
        to_sibling[r].start()
    for copies in (a2, b2):
        copies[2].wait_recv()
    x_ring[2].wait_recv()
    for copy in to_sibling:
        copy.wait_recv()
    backs = []
    rows = mx[...].reshape(192, 2048)
    for n in range(8):
        total = jnp.zeros((192, 256), jnp.float32)
        for r in range(4):
            near = wout[r, :, 256 * n : 256 * n + 256]
            spread = wplane[r, :, :, :, 256 * n : 256 * n + 256].reshape(256, 256)
            total += jnp.dot(rows[:, 512 * r : 512 * r + 256], near, preferred_element_type=jnp.float32)
            total += jnp.dot(rows[:, 512 * r + 256 : 512 * r + 512], spread, preferred_element_type=jnp.float32)
        total = total.astype(jnp.bfloat16)
        columns = pl.ds(pl.multiple_of(2048 * c + 256 * n, 256), 256)
        so[n] = total[96:]
        back = remote(so.at[n], out_ref.at[:, columns], ms.at[4 + n], mr.at[4 + n], sibling)
        back.start()
        backs.append(back)
        out_ref[:, columns] = total[:96]
    for back in backs:
        back.wait()
    for copy in to_sibling:
        copy.wait_send()
    for i in range(4):
        for rel, copy in enumerate(sends(i)):
            unless_own(i, rel, copy.wait_send)
    for copies in (a1, b1, a2, b2, x_ring):
        for copy in copies:
            copy.wait_send()
    for r in range(len(runs)):
        @pl.when(lax.rem(z, 2) == 1)
        def _():
            q_copies[r, 0].wait_send()

        for d in range(1, 4):
            z_copies[r, d].wait_send()
            q_copies[r, d].wait_send()
        if r != fine:
            for d in range(4):
                side_copies[r, d].wait_send()
            up_copies[r].wait_send()
            down_copies[r].wait_send()
            far_copies[r].wait_send()
        if runs[r][0]:
            g_copies[r].wait_send()
    for d in range(4):
        for copy in (fine_up[d], fine_down[d], fine_far[d], *(fine_side[d, k] for k in range(4))):
            copy.wait_send()
    for copy in slice_copies + to_right + to_left + far:
        copy.wait_send()


def layer(tokens, norm_gain, query_gain, key_gain, wq, wk, wv, wg, wo, offset, gain):
    vm = pl.BlockSpec(memory_space=pltpu.VMEM)
    hbm = pl.BlockSpec(memory_space=pltpu.HBM)
    smem = pl.BlockSpec(memory_space=pltpu.SMEM)
    count = sum(len(run) for run in RUNS)
    sems = pltpu.SemaphoreType.DMA
    half, full = jnp.bfloat16, jnp.float32
    return pl.pallas_call(
        layer_kernel,
        out_shape=jax.ShapeDtypeStruct((96, 4096), jnp.bfloat16),
        in_specs=[hbm, vm, vm, vm, hbm, hbm, hbm, hbm, hbm, vm, smem],
        out_specs=vm,
        scratch_shapes=[
            pltpu.VMEM((4, 8, 192, 512), half),
            pltpu.VMEM((4, NQ, 128), half),
            pltpu.VMEM((4, 96, 512), half),
            pltpu.VMEM((4, 16, 2048), half),
            pltpu.VMEM((4, 256, 2048), half),
            pltpu.VMEM((4, 4, 4, 16, 2048), half),
            pltpu.VMEM((4, 4, 96, 128), half),
            pltpu.VMEM((4, NQ, 128), half),
            pltpu.VMEM((2, 96, 2048), half),
            pltpu.VMEM((8, 96, 256), half),
            pltpu.VMEM((NQ, 128), full),
            pltpu.VMEM((NQ, 128), full),
            pltpu.VMEM((2, NQ, KP), half),
            pltpu.VMEM((2, NQ, KP), full),
            pltpu.VMEM((2, NQ, KP), full),
            pltpu.VMEM((2, NQ, KP), full),
            pltpu.VMEM((KP, KP), half),
            pltpu.VMEM((4, 96, 4096), half),
            pltpu.VMEM((96, 4096), half),
            pltpu.VMEM((8, 4096, 256), half),
            pltpu.VMEM((4, 4, 48, 512), half),
            pltpu.VMEM((4, 4, 96, 128), half),
            pltpu.VMEM((3, 96, 512), half),
            sems((10,)), sems((12,)), sems((12,)),
            sems((count, 4)), sems((count, 4)),
            sems((count, 7)), sems((count, 7)),
            sems((count, 4)), sems((count, 4)),
            sems((count,)), sems((count,)),
            sems((4, 7)), sems((4, 7)),
            sems((17,)), sems((5, 3)), sems((5, 3)),
            sems((4, 4)), sems((4, 4)), sems((12,)), sems((12,)),
        ],
        compiler_params=pltpu.CompilerParams(collective_id=0, has_side_effects=True, vmem_limit_bytes=56 * 2**20),
    )(tokens, norm_gain.reshape(1, -1), query_gain.reshape(1, -1), key_gain.reshape(1, -1), wq, wk, wv, wg, wo, gain.reshape(4, 1, 128), offset)


def on_device(tokens, norm_gain, query_weight, key_weight, value_weight, gate_weight, query_gain, key_gain, score_offset, out_gain, out_weight):
    return layer(tokens, norm_gain, query_gain, key_gain, query_weight, key_weight, value_weight, gate_weight, out_weight, score_offset, out_gain)


def solution(mesh):
    finer = Mesh(mesh.devices.reshape(4, 4, 2, mesh.shape["tp"]), ("sp_0", "sp_1", "sp_2", "tp"))
    in_specs = (P(SP_TP, None), P(), P(None, "tp"), P(None, "tp"), P(None, "tp"), P(None, "tp"), P(), P(), P("tp"), P("tp"), P("tp", None))
    return jax.shard_map(on_device, mesh=finer, in_specs=in_specs, out_specs=P(SP_TP, None), check_vma=False)
```
